512 devices in a mesh: sp: 128 (over z, x, core), tp: 4 (over y).
Axes of the slice: x: 4, y: 4, z: 16, core: 2. Of those that a mesh axis runs over, the one named last changes fastest.
Arguments:
- stream: bfloat16 [16384, 2048], P('sp', 'tp'), may hold values from -6 to 6
- norm_gain: float32 [2048], replicated, may hold values from 0.1 to 1.9
- w_query: bfloat16 [2048, 1024], P('sp', 'tp'), may hold values from -0.75 to 0.75
- w_key: bfloat16 [2048, 256], P('sp', 'tp'), may hold values from -0.125 to 0.125
- w_value: bfloat16 [2048, 256], P('sp', 'tp'), may hold values from -0.125 to 0.125
- w_conv_in: bfloat16 [2048, 1024], P('sp', 'tp'), may hold values from -0.125 to 0.125
- w_conv_gate: bfloat16 [2048, 1024], P('sp', 'tp'), may hold values from -0.125 to 0.125
- conv_taps: float32 [3, 1024], P(None, 'tp'), may hold values from -3.5 to 3.5
- sb_bias: float32 [16], P('tp'), may hold values from -28 to -13
- w_out_attn: bfloat16 [1024, 2048], P('tp', 'sp'), may hold values from -0.5 to 0.5
- w_out_conv: bfloat16 [1024, 2048], P('tp', 'sp'), may hold values from -0.125 to 0.125
Outputs:
- mixed: bfloat16 [16384, 2048], P('sp', 'tp')
- log_weight_sum: float32 [16, 16384], P('tp', 'sp')
The draws below stay inside these ranges and needn't reach their ends.
All inputs are finite; a program needn't handle non-finite values.
Results may differ from the reference program's by a relative error of at most 0.013.
The reference program's roundings to bfloat16 on the way count: a program that leaves them out, or rounds other values in their place, can miss the bound.
Values may be sent and summed in bfloat16 or wider, within the bound.
A program may use at most 64 MiB of HBM per device.

```python
import math
import jax
import jax.numpy as jnp
from jax import lax

D = 2048
HEADS = 16
HEAD = 64
KV_HEADS = 4
CONV = 1024
CONV_K = 3
SEQ = 16384
N_TP = 4


def draw_sb_bias(key, part):
    pick_key, slow_key, fast_key = jax.random.split(jax.random.fold_in(key, 11), 3)
    reach = math.sqrt(2.0 * math.log(SEQ)) - 0.4
    share = 0.5
    quick = jax.random.uniform(pick_key, (HEADS,), jnp.float32) < share
    slow = -6.0 * reach + jax.random.uniform(slow_key, (HEADS,), jnp.float32, -1.0, 1.0)
    fast = -14.0 + jax.random.uniform(fast_key, (HEADS,), jnp.float32, -1.0, 1.0)
    return jnp.where(quick, fast, slow).astype(jnp.float32)


def steps_of(own_key, shape, pieces, low, high):
    factor_of, own = 1.0, jax.random.fold_in(own_key, 6)
    for dim, shards_of in pieces:
        steps = jnp.exp(jax.random.uniform(jax.random.fold_in(own, dim), (shards_of,), jnp.float32, low / len(pieces), high / len(pieces)))
        factor_of = factor_of * jnp.repeat(steps, shape[dim] // shards_of).reshape([-1 if axis == dim else 1 for axis in range(len(shape))])
    return factor_of


def scatter_about(rng, dims, width, most, cuts=(), kind=jnp.bfloat16):
    array = width * jax.random.normal(rng, dims, jnp.float32)
    if cuts:
        array = array * steps_of(rng, dims, cuts, -0.22, 0.18)
    return jnp.clip(array, -most, most).astype(kind)


def setup_inputs(seed: int = 0) -> dict:
    streams_of = jax.random.split(jax.random.key(seed), 12)
    return {
        "stream": scatter_about(streams_of[0], (SEQ, D), 1.0, 6.0, ((0, 128), (1, 4))),
        "norm_gain": jnp.clip(1.0 + 0.18 * jax.random.normal(streams_of[1], (D,), jnp.float32), 0.1, 1.9),
        "w_query": scatter_about(streams_of[2], (D, HEADS * HEAD), (D // 36) ** -0.5, 0.75, ((0, 128), (1, 4))),
        "w_key": scatter_about(streams_of[3], (D, KV_HEADS * HEAD), D ** -0.5, 0.125, ((0, 128), (1, 4))),
        "w_value": scatter_about(streams_of[4], (D, KV_HEADS * HEAD), D ** -0.5, 0.125, ((0, 128), (1, 4))),
        "w_conv_in": scatter_about(streams_of[5], (D, CONV), D ** -0.5, 0.125, ((0, 128), (1, 4))),
        "w_conv_gate": scatter_about(streams_of[6], (D, CONV), D ** -0.5, 0.125, ((0, 128), (1, 4))),
        "conv_taps": scatter_about(streams_of[7], (CONV_K, CONV), CONV_K ** -0.5, 3.5, ((1, 4),), jnp.float32),
        "sb_bias": draw_sb_bias(jax.random.fold_in(streams_of[11], 71), 0),
        "w_out_attn": scatter_about(streams_of[9], (HEADS * HEAD, D), (HEADS * HEAD // 8) ** -0.5, 0.5, ((0, 4), (1, 128))),
        "w_out_conv": scatter_about(streams_of[10], (CONV, D), (2 * CONV) ** -0.5, 0.125, ((0, 4), (1, 128))),
    }


EPS = 1e-06
FLOOR = 0.02

def project(scaled, weight, row_scale):
    return (jnp.dot(scaled, weight, preferred_element_type=jnp.float32) * row_scale).astype(jnp.bfloat16)

def reference(stream, norm_gain, w_query, w_key, w_value, w_conv_in, w_conv_gate, conv_taps, sb_bias, w_out_attn, w_out_conv):
    stream_f = stream.astype(jnp.float32)
    row_scale = lax.rsqrt(lax.optimization_barrier(jnp.mean(stream_f * stream_f, axis=1, keepdims=True)) + EPS)
    scaled = (stream_f * norm_gain[None, :]).astype(jnp.bfloat16)
    query = project(scaled, w_query, row_scale)
    key = project(scaled, w_key, row_scale)
    value = project(scaled, w_value, row_scale)
    conv_in = project(scaled, w_conv_in, row_scale)
    conv_gate = project(scaled, w_conv_gate, row_scale)
    group = HEADS // KV_HEADS
    queries = query.reshape(SEQ, HEADS, HEAD).transpose(1, 0, 2).astype(jnp.float32)
    keys = jnp.repeat(key.reshape(SEQ, KV_HEADS, HEAD).transpose(1, 0, 2), group, axis=0).astype(jnp.float32)
    values = jnp.repeat(value.reshape(SEQ, KV_HEADS, HEAD).transpose(1, 0, 2), group, axis=0).astype(jnp.float32)
    block = min(512, SEQ)
    blocks = SEQ // block
    score_scale = HEAD ** (-0.5)

    def query_block(block_index):
        begin = (block_index * block).astype(jnp.int32)
        query_rows = lax.dynamic_slice_in_dim(queries, begin, block, 1)
        query_pos = begin + jnp.arange(block, dtype=jnp.int32)

        def turn(step, carry):
            totals, survival = carry
            start = ((block_index - step) * block).astype(jnp.int32)
            key_rows = lax.dynamic_slice_in_dim(keys, start, block, 1)
            value_rows = lax.dynamic_slice_in_dim(values, start, block, 1)
            key_pos = start + jnp.arange(block, dtype=jnp.int32)
            causal = (key_pos[None, :] < query_pos[:, None])[None]
            scores = jnp.einsum('hqd,hkd->hqk', query_rows, key_rows) * score_scale + sb_bias[:, None, None]
            fails = jnp.where(causal, jax.nn.log_sigmoid(-scores), 0.0)
            later = lax.cumsum(fails, axis=2, reverse=True) - fails + survival[:, :, None]
            stick = jnp.where(causal, jnp.exp(jax.nn.log_sigmoid(scores) + later), 0.0)
            stick = lax.optimization_barrier(stick.astype(jnp.bfloat16)).astype(jnp.float32)
            totals = totals + jnp.einsum('hqk,hkd->hqd', stick, value_rows)
            return (totals, survival + lax.optimization_barrier(jnp.sum(fails, axis=2)))
        start_state = (jnp.zeros((HEADS, block, HEAD), jnp.float32), jnp.zeros((HEADS, block), jnp.float32))
        return lax.fori_loop(0, block_index + 1, turn, start_state)
    totals, survival = lax.map(query_block, jnp.arange(blocks, dtype=jnp.int32))
    attended = totals.transpose(1, 0, 2, 3).reshape(HEADS, SEQ, HEAD).astype(jnp.bfloat16)
    survival = survival.transpose(1, 0, 2).reshape(HEADS, SEQ)
    log_weight_sum = jnp.log(jnp.maximum(-jnp.expm1(survival), FLOOR))
    padded = jnp.pad(conv_in.astype(jnp.float32), ((CONV_K - 1, 0), (0, 0)))
    conv_mixed = jnp.zeros((SEQ, CONV), jnp.float32)
    for tap in range(CONV_K):
        conv_mixed = conv_mixed + conv_taps[tap][None, :] * padded[tap:tap + SEQ]
    conv_out = (conv_gate.astype(jnp.float32) * conv_mixed).astype(jnp.bfloat16)
    attended_rows = attended.transpose(1, 0, 2).reshape(SEQ, HEADS * HEAD)
    attn_width = HEADS * HEAD // N_TP
    conv_width = CONV // N_TP
    summed = jnp.zeros((SEQ, D), jnp.float32)
    for group_index in range(N_TP):
        lower = group_index * attn_width
        conv_lower = group_index * conv_width
        partial_value = jnp.dot(attended_rows[:, lower:lower + attn_width], w_out_attn[lower:lower + attn_width], preferred_element_type=jnp.float32)
        partial_value = partial_value + jnp.dot(conv_out[:, conv_lower:conv_lower + conv_width], w_out_conv[conv_lower:conv_lower + conv_width], preferred_element_type=jnp.float32)
        summed = summed + lax.optimization_barrier(partial_value.astype(jnp.bfloat16)).astype(jnp.float32)
    return (summed.astype(jnp.bfloat16), log_weight_sum)
```

```python
import functools

import jax
import jax.numpy as jnp
from jax import lax
from jax.experimental import pallas as pl
from jax.experimental.pallas import tpu as pltpu
from jax.sharding import Mesh
from jax.sharding import PartitionSpec as P

D = 2048
HEAD = 64
CONV_K = 3
SP = ("sp_0", "sp_1", "sp_2")
KEYS = 256
EPS = 1e-06
FLOOR = 0.02
MESH = pl.DeviceIdType.MESH


def gather_kernel(nz, in_ref, out_ref, zs, zr, xs, xr, ps, pr):
    z, x, c = (lax.axis_index(a) for a in SP)
    nx = 4
    ups, downs = nz // 2, (nz - 1) // 2
    z_up, z_down = {"sp_0": lax.rem(z + 1, nz)}, {"sp_0": lax.rem(z + nz - 1, nz)}
    x_up, x_down = {"sp_1": lax.rem(x + 1, nx)}, {"sp_1": lax.rem(x + nx - 1, nx)}
    partner = {"sp_2": 1 - c}
    barrier = pltpu.get_barrier_semaphore()
    for peer in (z_up, z_down, x_up, x_down, partner):
        pl.semaphore_signal(barrier, inc=1, device_id=peer, device_id_type=MESH)
    pl.semaphore_wait(barrier, 5)

    def plane(dz):
        return lax.rem(z + dz + nz, nz)

    def column(dx):
        return lax.rem(x + dx + nx, nx)

    def index_of(dz):
        return -dz if dz <= 0 else ups + dz

    def copy(src, dst, ssem, rsem, peer):
        return pltpu.make_async_remote_copy(
            src_ref=src, dst_ref=dst, send_sem=ssem, recv_sem=rsem, device_id=peer, device_id_type=MESH
        )

    out_ref[z, x, c] = in_ref[...]
    sends = []

    def send(src, dst, ssem, rsem, peer):
        one = copy(src, dst, ssem, rsem, peer)
        one.start()
        sends.append(one)

    def await_block(slot, ssem, rsem, peer):
        copy(slot, slot, ssem, rsem, peer).wait_recv()

    def new_at(step):
        if step == 0:
            return [0]
        return ([-step] if step <= ups else []) + ([step] if 0 < step <= downs else [])

    for step in range(ups + 3):
        for dz in new_at(step):
            k = index_of(dz)
            slot = out_ref.at[plane(dz), x, c]
            if dz < 0:
                await_block(slot, zs.at[k], zr.at[k], z_down)
            elif dz > 0:
                await_block(slot, zs.at[k], zr.at[k], z_up)
            src = in_ref if dz == 0 else slot
            if dz <= 0 and step < ups:
                n = index_of(dz - 1)
                send(src, slot, zs.at[n], zr.at[n], z_up)
            if dz >= 0 and step < downs:
                n = index_of(dz + 1)
                send(src, slot, zs.at[n], zr.at[n], z_down)
            send(src, slot, xs.at[k, 0], xr.at[k, 0], x_up)
            send(src, slot, xs.at[k, 1], xr.at[k, 1], x_down)
        for dz in new_at(step - 1) if step >= 1 else []:
            k = index_of(dz)
            left = out_ref.at[plane(dz), column(-1), c]
            right = out_ref.at[plane(dz), column(1), c]
            await_block(left, xs.at[k, 0], xr.at[k, 0], x_down)
            await_block(right, xs.at[k, 1], xr.at[k, 1], x_up)
            if dz <= 0:
                send(left, left, xs.at[k, 2], xr.at[k, 2], x_up)
            else:
                send(right, right, xs.at[k, 2], xr.at[k, 2], x_down)
        for dz in new_at(step - 2) if step >= 2 else []:
            k = index_of(dz)
            far = out_ref.at[plane(dz), column(2), c]
            await_block(far, xs.at[k, 2], xr.at[k, 2], x_down if dz <= 0 else x_up)
            row = out_ref.at[plane(dz), :, c]
            send(row, row, ps.at[k], pr.at[k], partner)
    for k, dz in enumerate([*range(0, -ups - 1, -1), *range(1, downs + 1)]):
        row = out_ref.at[plane(dz), :, 1 - c]
        await_block(row, ps.at[k], pr.at[k], partner)
    for one in sends:
        one.wait_send()


def gather(block, nz, collective_id):
    rows, cols = block.shape
    dma = pltpu.SemaphoreType.DMA
    return pl.pallas_call(
        functools.partial(gather_kernel, nz),
        name="gather_sp",
        out_shape=jax.ShapeDtypeStruct((nz, 4, 2, rows, cols), block.dtype),
        in_specs=[pl.BlockSpec(memory_space=pltpu.VMEM)],
        out_specs=pl.BlockSpec(memory_space=pltpu.VMEM),
        scratch_shapes=[dma((nz,)), dma((nz,)), dma((nz, 3)), dma((nz, 3)), dma((nz,)), dma((nz,))],
        compiler_params=pltpu.CompilerParams(collective_id=collective_id, has_side_effects=True),
    )(block).reshape(-1, cols)


def sweep_kernel(bias_ref, q_ref, kv_ref, tri_ref, o_ref, s_ref):
    me = (lax.axis_index(SP[0]) * 4 + lax.axis_index(SP[1])) * 2 + lax.axis_index(SP[2])
    heads = bias_ref.shape[0]
    rows = q_ref.shape[0] // heads
    o_ref[...] = jnp.zeros_like(o_ref)
    s_ref[...] = jnp.zeros_like(s_ref)

    def block(begin, masked):
        kv = kv_ref[pl.ds(begin, KEYS), :]
        for h in range(heads):
            part = pl.ds(h * rows, rows)
            score = (
                lax.dot_general(
                    q_ref[part, :], kv, (((1,), (1,)), ((), ())), preferred_element_type=jnp.float32
                )
                + bias_ref[h]
            )
            if masked:
                key_pos = begin + lax.broadcasted_iota(jnp.int32, score.shape, 1)
                query_pos = me * rows + lax.broadcasted_iota(jnp.int32, score.shape, 0)
                score = jnp.where(key_pos < query_pos, score, -1e30)
            soft = jnp.log(1.0 + jnp.exp(-jnp.abs(score)))
            fail = jnp.maximum(score, 0.0) + soft
            high = fail.astype(jnp.bfloat16)
            low = (fail - high.astype(jnp.float32)).astype(jnp.bfloat16)
            tri = tri_ref[...]
            later = jnp.dot(high, tri, preferred_element_type=jnp.float32) + jnp.dot(
                low, tri, preferred_element_type=jnp.float32
            )
            stick = jnp.exp(jnp.minimum(score, 0.0) - soft - later).astype(jnp.bfloat16)
            out = jnp.dot(stick, kv, preferred_element_type=jnp.float32)
            gone = s_ref[part, :]
            o_ref[part, :] += jnp.exp(-gone) * out
            s_ref[part, :] = gone + (later[:, :1] + fail[:, :1])

    per_turn = 2 * KEYS // rows
    turns = lax.div(me, per_turn)
    for half in (1, 0):
        block(pl.multiple_of(turns * 2 * KEYS + half * KEYS, KEYS), True)

    @pl.loop(0, turns)
    def _(turn):
        for half in (1, 0):
            block(pl.multiple_of((turns - 1 - turn) * 2 * KEYS + half * KEYS, KEYS), False)


def sweep(query, all_kv, sb_bias):
    tokens, heads = query.shape[0], query.shape[1] // HEAD
    q = (query * HEAD ** (-0.5)).astype(jnp.bfloat16).reshape(tokens, heads, HEAD).transpose(1, 0, 2)
    q = jnp.pad(q.reshape(heads * tokens, HEAD), ((0, 0), (0, HEAD)))
    order = jnp.arange(KEYS)
    tri = (order[:, None] > order[None, :]).astype(jnp.bfloat16)
    vmem = pl.BlockSpec(memory_space=pltpu.VMEM)
    wide = jax.ShapeDtypeStruct((heads * tokens, 2 * HEAD), jnp.float32)
    out, gone = pl.pallas_call(
        sweep_kernel,
        name="sweep",
        out_shape=(wide, wide),
        in_specs=[pl.BlockSpec(memory_space=pltpu.SMEM), vmem, vmem, vmem],
        out_specs=(vmem, vmem),
    )(sb_bias, q, all_kv, tri)
    attended = out[:, HEAD:].astype(jnp.bfloat16).reshape(heads, tokens, HEAD)
    survival = -gone[:, 0].reshape(heads, tokens)
    return attended.transpose(1, 0, 2).reshape(tokens, heads * HEAD), survival


def copy_for_each(value, axis):
    copies = jnp.broadcast_to(value, (lax.axis_size(axis), *value.shape))
    return lax.all_to_all(copies, axis, split_axis=0, concat_axis=0, tiled=True)


def collect(value, axis):
    parts = copy_for_each(value, axis)
    return jnp.moveaxis(parts, 0, 1).reshape(value.shape[0], -1)


def from_behind(value, axis, steps):
    count = lax.axis_size(axis)
    return lax.ppermute(value, axis, [(source, source + steps) for source in range(count - steps)])


def summed_on_arrival(value, axis):
    size = lax.axis_size(axis)
    rows, cols = value.shape
    parts = jnp.moveaxis(value.reshape(rows, size, cols // size), 1, 0)
    parts = lax.all_to_all(parts, axis, 0, 0, tiled=True)
    return jnp.sum(parts.astype(jnp.float32), axis=0)


def local(
    stream,
    norm_gain,
    w_query,
    w_key,
    w_value,
    w_conv_in,
    w_conv_gate,
    conv_taps,
    sb_bias,
    w_out_attn,
    w_out_conv,
):
    tokens = stream.shape[0]
    nz = lax.axis_size(SP[0])
    ins = (w_key, w_value, w_query, w_conv_in, w_conv_gate)
    held = jnp.concatenate([*ins, w_out_attn.T, w_out_conv.T], axis=1)
    weights = gather(held, nz, 0)
    piece_f = collect(stream, "tp").astype(jnp.float32)
    scaled = (piece_f * norm_gain[None, :]).astype(jnp.bfloat16)
    row_scale = lax.rsqrt(jnp.sum(piece_f * piece_f, axis=1) / D + EPS)[:, None]
    ends, at = [], 0
    for w in ins:
        at += w.shape[1]
        ends.append(at)
    sums = jnp.dot(scaled, weights[:, :at], preferred_element_type=jnp.float32)
    mine = (sums * row_scale).astype(jnp.bfloat16)
    kv = mine[:, : ends[1]]
    query, conv_in, conv_gate = jnp.split(mine[:, ends[1] :], [e - ends[1] for e in ends[2:4]], axis=1)
    all_kv = gather(kv, nz, 1)
    previous = from_behind(conv_in[tokens - (CONV_K - 1) :], SP, 1)
    padded = jnp.concatenate([previous, conv_in], axis=0).astype(jnp.float32)
    conv_mixed = jnp.zeros((tokens, conv_in.shape[1]), jnp.float32)
    for tap in range(CONV_K):
        conv_mixed = conv_mixed + conv_taps[tap][None, :] * padded[tap : tap + tokens]
    conv_out = (conv_gate.astype(jnp.float32) * conv_mixed).astype(jnp.bfloat16)
    attended, survs = sweep(query, all_kv, sb_bias)
    log_weight_sum = jnp.log(jnp.maximum(-jnp.expm1(survs), FLOOR))
    partial_value = lax.dot_general(
        jnp.concatenate([attended, conv_out], axis=1),
        weights[:, at:],
        (((1,), (1,)), ((), ())),
        preferred_element_type=jnp.float32,
    )
    mixed = summed_on_arrival(partial_value.astype(jnp.bfloat16), "tp").astype(jnp.bfloat16)
    return (mixed, log_weight_sum)


def solution(mesh):
    torus = Mesh(
        mesh.devices.reshape(mesh.shape["sp"] // 8, 4, 2, mesh.shape["tp"]),
        ("sp_0", "sp_1", "sp_2", "tp"),
    )
    return jax.shard_map(
        local,
        mesh=torus,
        in_specs=(
            P(SP, "tp"),
            P(),
            P(SP, "tp"),
            P(SP, "tp"),
            P(SP, "tp"),
            P(SP, "tp"),
            P(SP, "tp"),
            P(None, "tp"),
            P("tp"),
            P("tp", SP),
            P("tp", SP),
        ),
        out_specs=(P(SP, "tp"), P("tp", SP)),
        check_vma=False,
    )
```

```python
import functools

import jax
import jax.numpy as jnp
from jax import lax
from jax.experimental import pallas as pl
from jax.experimental.pallas import tpu as pltpu
from jax.sharding import Mesh
from jax.sharding import PartitionSpec as P

HEAD = 64
SP = ("sp_0", "sp_1", "sp_2")
KEYS = 256
EPS = 1e-06
FLOOR = 0.02
LN2 = 0.6931471805599453
NT = (((1,), (1,)), ((), ()))
MESH = pl.DeviceIdType.MESH


class Spread:
    def __init__(self, nz, own, buf, zs, zr, xs, xr, ps, pr):
        self.nz, self.own, self.buf = nz, own, buf
        self.zs, self.zr, self.xs, self.xr, self.ps, self.pr = zs, zr, xs, xr, ps, pr
        self.z, self.x, self.c = (lax.axis_index(a) for a in SP)
        self.ups, self.downs = nz // 2, (nz - 1) // 2
        self.z_up, self.z_down = ({"sp_0": lax.rem(self.z + d, nz)} for d in (1, nz - 1))
        self.x_up, self.x_down = ({"sp_1": lax.rem(self.x + d, 4)} for d in (1, 3))
        self.partner = {"sp_2": 1 - self.c}
        self.peers = (self.z_up, self.z_down, self.x_up, self.x_down, self.partner)

    def plane(self, up, n):
        return lax.rem(self.z - n + self.nz, self.nz) if up else lax.rem(self.z + n, self.nz)

    def slot(self, up, n, dx=0):
        return self.buf.at[self.plane(up, n), lax.rem(self.x + dx, 4), self.c]

    def index(self, up, n):
        return n if up else self.ups + n

    def on_z(self, up, n, src=None):
        k, slot = self.index(up, n), self.slot(up, n)
        return remote(slot if src is None else src, slot, self.zs.at[k], self.zr.at[k], self.z_up if up else self.z_down)

    def passed_on(self, up, n, src):
        k, slot = self.index(up, n + 1), self.slot(up, n)
        return remote(src, slot, self.zs.at[k], self.zr.at[k], self.z_up if up else self.z_down)

    def along_x(self, up, n, way, src=None):
        k, slot = self.index(up, n), self.slot(up, n)
        peer = self.x_up if way == 0 else self.x_down
        return remote(slot if src is None else src, slot, self.xs.at[k, way], self.xr.at[k, way], peer)

    def far_x(self, up, n):
        k, slot = self.index(up, n), self.slot(up, n, 3 if up else 1)
        return remote(slot, slot, self.xs.at[k, 2], self.xr.at[k, 2], self.x_up if up else self.x_down)

    def across(self, up, n, core):
        k, row = self.index(up, n), self.buf.at[self.plane(up, n), :, core]
        return remote(row, row, self.ps.at[k], self.pr.at[k], self.partner)

    def each(self, n, work):
        when(n <= self.ups, lambda: work(True))
        when(n <= self.downs, lambda: work(False))

    def begin(self):
        own = self.own
        self.passed_on(True, 0, own).start()
        if self.downs:
            self.passed_on(False, 0, own).start()
        self.along_x(True, 0, 0, own).start()
        self.along_x(True, 0, 1, own).start()
        self.buf[self.z, self.x, self.c] = own[...]

    def step_z(self, n):
        def work(up):
            self.on_z(up, n).wait_recv()
            when(n < (self.ups if up else self.downs), lambda: self.passed_on(up, n, self.slot(up, n)).start())
            for way in (0, 1):
                self.along_x(up, n, way).start()

        self.each(n, work)

    def step_x(self, n, first=False):
        def work(up):
            for way in (0, 1):
                self.along_x(up, n, way).wait_recv()
            self.far_x(up, n).start()

        work(True) if first else self.each(n, work)

    def step_far(self, n, first=False):
        def work(up):
            self.far_x(up, n).wait_recv()
            self.across(up, n, self.c).start()

        work(True) if first else self.each(n, work)

    def step_across(self, n, first=False):
        def work(up):
            self.across(up, n, 1 - self.c).wait_recv()

        work(True) if first else self.each(n, work)

    def finish(self):
        for k in range(self.nz):
            up = k <= self.ups
            n = k if up else k - self.ups
            if k:
                self.on_z(up, n).wait_send()
            for way in (0, 1):
                self.along_x(up, n, way).wait_send()
            self.far_x(up, n).wait_send()
            self.across(up, n, self.c).wait_send()


def remote(src, dst, ssem, rsem, peer):
    return pltpu.make_async_remote_copy(
        src_ref=src, dst_ref=dst, send_sem=ssem, recv_sem=rsem, device_id=peer, device_id_type=MESH
    )


def when(cond, work):
    if isinstance(cond, bool):
        if cond:
            work()
    else:
        pl.when(cond)(work)


def greet(peers):
    barrier = pltpu.get_barrier_semaphore()
    for peer in peers:
        pl.semaphore_signal(barrier, inc=1, device_id=peer, device_id_type=MESH)
    pl.semaphore_wait(barrier, len(peers))


def gather_kernel(nz, in_ref, out_ref, *sems):
    net = Spread(nz, in_ref, out_ref, *sems)
    greet(net.peers)
    net.begin()
    for step in range(1, net.ups + 6):
        net.step_z(step)
        if step >= 2:
            net.step_x(step - 2, step == 2)
        if step >= 4:
            net.step_far(step - 4, step == 4)
    for step in range(net.ups + 1):
        net.step_across(step, step == 0)
    net.finish()


def spread_sems(nz):
    dma = pltpu.SemaphoreType.DMA
    return [dma((nz,)), dma((nz,)), dma((nz, 3)), dma((nz, 3)), dma((nz,)), dma((nz,))]


def gather(block, nz, collective_id):
    rows, cols = block.shape
    return pl.pallas_call(
        functools.partial(gather_kernel, nz),
        name="gather_sp",
        out_shape=jax.ShapeDtypeStruct((nz, 4, 2, rows, cols), block.dtype),
        in_specs=[pl.BlockSpec(memory_space=pltpu.VMEM)],
        out_specs=pl.BlockSpec(memory_space=pltpu.VMEM),
        scratch_shapes=spread_sems(nz),
        compiler_params=pltpu.CompilerParams(collective_id=collective_id, has_side_effects=True),
    )(block).reshape(-1, cols)


def attend_kernel(
    nz, nt, bias_ref, q_ref, own_ref, conv_ref, gate_ref, taps_ref, tri_ref, mixed_ref, weight_ref,
    buf, halo, o_new, s_new, o_old, s_old, part, heard, zs, zr, xs, xr, ps, pr, hs, hr, ys, yr,
):
    net = Spread(nz, own_ref, buf, zs, zr, xs, xr, ps, pr)
    me = (net.z * 4 + net.x) * 2 + net.c
    y = lax.axis_index("tp")
    heads = bias_ref.shape[0]
    rows = q_ref.shape[0] // heads
    total = nz * 8

    def device(index):
        return {"sp_0": lax.div(index, 8), "sp_1": lax.rem(lax.div(index, 2), 4), "sp_2": lax.rem(index, 2)}

    ahead, behind = device(lax.rem(me + 1, total)), device(lax.rem(me + total - 1, total))
    others = [{"tp": lax.rem(y + r, nt)} for r in range(1, nt)]
    greet((*net.peers, ahead, behind, *others))
    net.begin()
    tail = remote(conv_ref.at[pl.ds(rows - 16, 16), :], halo, hs, hr, ahead)
    tail.start()
    for ref in (o_new, s_new, o_old, s_old):
        ref[...] = jnp.zeros_like(ref)

    def sweep(at, masked):
        out, gone = None, None
        for i in (3, 2, 1, 0):
            kv = buf[at, i, :, pl.ds(0, rows), :].reshape(KEYS, 2 * HEAD)
            both = jnp.concatenate([kv[:, :HEAD], kv[:, :HEAD]], axis=1)
            score = lax.dot_general(q_ref[...], both, NT, preferred_element_type=jnp.float32)
            score = jnp.concatenate(
                [score[h * rows : (h + 1) * rows] + bias_ref[h] for h in range(heads)], axis=0
            )
            if masked:
                key_pos = i * KEYS + lax.broadcasted_iota(jnp.int32, score.shape, 1)
                query_pos = lax.rem(me, 8) * rows + lax.rem(
                    lax.broadcasted_iota(jnp.int32, score.shape, 0), rows
                )
                score = jnp.where(key_pos < query_pos, score, -1e30)
            fail = jnp.maximum(score, lax.log2(1.0 + jnp.exp2(jnp.minimum(score, 80.0))))
            later = jnp.dot(fail.astype(jnp.bfloat16), tri_ref[...], preferred_element_type=jnp.float32)
            power = (score - fail) - later
            block = later[:, :1] + fail[:, :1]
            if gone is None:
                gone = jnp.broadcast_to(block, (heads * rows, 2 * HEAD))
            else:
                power = power - jnp.concatenate([gone, gone], axis=1)
                gone = gone + block
            stick = jnp.exp2(power).astype(jnp.bfloat16)
            term = jnp.dot(stick, kv, preferred_element_type=jnp.float32)
            out = term if out is None else out + term
        return out, gone

    def take_new(n, masked=False):
        out, gone = sweep(net.plane(True, n), masked)
        before = s_new[...]
        o_new[...] += jnp.exp2(-before) * out
        s_new[...] = before + gone

    def take_old(n):
        out, gone = sweep(net.plane(False, n), False)
        o_old[...] = o_old[...] * jnp.exp2(-gone) + out
        s_old[...] += gone

    net.step_z(1)
    net.step_x(0, True)
    net.step_z(2)
    net.step_x(1)
    net.step_far(0, True)
    net.step_z(3)
    net.step_across(0, True)
    take_new(0, True)
    net.step_x(2)
    net.step_far(1)

    @pl.loop(1, net.ups + 1)
    def _(n):
        net.step_z(n + 3)
        net.step_across(n)
        pl.when(net.z - n >= 0)(lambda: take_new(n))
        net.step_x(n + 2)
        pl.when((net.z + n >= nz) & (n <= net.downs))(lambda: take_old(n))
        net.step_far(n + 1)

    gone = s_new[...]
    out = o_new[...] + jnp.exp2(-gone) * o_old[...]
    survived = (gone + s_old[...]) * LN2
    weight = jnp.log(jnp.maximum(1.0 - jnp.exp(-survived), FLOOR))
    diagonal = lax.broadcasted_iota(jnp.int32, (rows, rows), 0) == lax.broadcasted_iota(
        jnp.int32, (rows, rows), 1
    )
    for h in range(heads):
        weight_ref[pl.ds(h, 1), :] = jnp.sum(
            jnp.where(diagonal, weight[h * rows : (h + 1) * rows], 0.0), axis=0, keepdims=True
        )
    attended = [out[h * rows : (h + 1) * rows, HEAD:] for h in range(heads)]

    tail.wait_recv()
    now = conv_ref[...].astype(jnp.float32)
    last = halo[...].astype(jnp.float32) * jnp.where(me > 0, 1.0, 0.0)
    row = lax.broadcasted_iota(jnp.int32, now.shape, 0)
    one = jnp.where(row == 0, last[15:16], pltpu.roll(now, 1, 0))
    two = jnp.where(row == 0, last[14:15], jnp.where(row == 1, last[15:16], pltpu.roll(now, 2, 0)))
    conv = taps_ref[0:1, :] * two + taps_ref[1:2, :] * one + taps_ref[2:3, :] * now
    conv = gate_ref[...].astype(jnp.float32) * conv
    act = jnp.concatenate([*attended, conv], axis=1).astype(jnp.bfloat16)

    share = nz // nt

    def project(to):
        planes = pl.ds(to * share, share)
        acc = None
        for j in range(4):
            w = buf[planes, :, :, pl.ds(rows + 16 * j, 16), :].reshape(share * 128, 128)
            term = lax.dot_general(
                act[:, 128 * j : 128 * (j + 1)], w, NT, preferred_element_type=jnp.float32
            )
            acc = term if acc is None else acc + term
        return acc.astype(jnp.bfloat16)

    sent = []
    for r in [*range(2, nt), 1] if nt > 1 else []:
        part[r] = project(lax.rem(y + r, nt))
        sent.append(remote(part.at[r], heard.at[r], ys.at[r], yr.at[r], others[r - 1]))
        sent[-1].start()
    mixed = project(y).astype(jnp.float32)
    for one_sent in sent:
        one_sent.wait_recv()
    for r in range(1, nt):
        mixed = mixed + heard[r].astype(jnp.float32)
    mixed_ref[...] = mixed.astype(jnp.bfloat16)
    for one_sent in sent:
        one_sent.wait_send()
    tail.wait_send()
    net.finish()


def attend(query, kv, w_out, conv_in, conv_gate, conv_taps, sb_bias, nz, nt):
    tokens, heads = query.shape[0], query.shape[1] // HEAD
    q = query.astype(jnp.float32).reshape(tokens, heads, HEAD).transpose(1, 0, 2) * (HEAD ** (-0.5) / LN2)
    q = q.reshape(heads * tokens, HEAD)
    high = lax.reduce_precision(q, 8, 7)
    q = jnp.concatenate([high, q - high], axis=1).astype(jnp.bfloat16)
    order = jnp.arange(KEYS)
    tri = (order[:, None] > order[None, :]).astype(jnp.bfloat16)
    cols = w_out.shape[0] // 4
    w_rows = w_out.reshape(4, cols, 16).transpose(0, 2, 1).reshape(64, cols)
    own = jnp.concatenate([kv, w_rows], axis=0)
    vmem = pl.BlockSpec(memory_space=pltpu.VMEM)
    out_cols = nz * 128 // nt
    wide = pltpu.VMEM((heads * tokens, 2 * HEAD), jnp.float32)
    parts = pltpu.VMEM((nt, tokens, out_cols), jnp.bfloat16)
    dma = pltpu.SemaphoreType.DMA
    return pl.pallas_call(
        functools.partial(attend_kernel, nz, nt),
        name="attend",
        out_shape=(
            jax.ShapeDtypeStruct((tokens, out_cols), jnp.bfloat16),
            jax.ShapeDtypeStruct((heads, tokens), jnp.float32),
        ),
        in_specs=[pl.BlockSpec(memory_space=pltpu.SMEM)] + [vmem] * 6,
        out_specs=(vmem, vmem),
        scratch_shapes=[
            pltpu.VMEM((nz, 4, 2, *own.shape), jnp.bfloat16),
            pltpu.VMEM((16, conv_in.shape[1]), jnp.bfloat16),
            *[wide] * 4,
            *[parts] * 2,
            *spread_sems(nz),
            dma,
            dma,
            dma((nt,)),
            dma((nt,)),
        ],
        compiler_params=pltpu.CompilerParams(collective_id=1, has_side_effects=True),
    )(sb_bias / LN2, q, own, conv_in, conv_gate, conv_taps, tri)


def copy_for_each(value, axis):
    copies = jnp.broadcast_to(value, (lax.axis_size(axis), *value.shape))
    return lax.all_to_all(copies, axis, split_axis=0, concat_axis=0, tiled=True)


def collect(value, axis):
    parts = copy_for_each(value, axis)
    return jnp.moveaxis(parts, 0, 1).reshape(value.shape[0], -1)


def local(
    stream,
    norm_gain,
    w_query,
    w_key,
    w_value,
    w_conv_in,
    w_conv_gate,
    conv_taps,
    sb_bias,
    w_out_attn,
    w_out_conv,
):
    nz, nt = lax.axis_size(SP[0]), lax.axis_size("tp")
    ins = (w_key, w_value, w_query, w_conv_in, w_conv_gate)
    weights = gather(jnp.concatenate(ins, axis=1), nz, 0)
    piece_f = collect(stream, "tp").astype(jnp.float32)
    scaled = (piece_f * norm_gain[None, :]).astype(jnp.bfloat16)
    row_scale = lax.rsqrt(jnp.sum(piece_f * piece_f, axis=1) / piece_f.shape[1] + EPS)[:, None]
    sums = jnp.dot(scaled, weights, preferred_element_type=jnp.float32)
    mine = (sums * row_scale).astype(jnp.bfloat16)
    ends, at = [], w_key.shape[1]
    for w in ins[1:-1]:
        at += w.shape[1]
        ends.append(at)
    kv, query, conv_in, conv_gate = jnp.split(mine, ends, axis=1)
    w_out = jnp.concatenate([w_out_attn, w_out_conv], axis=0)
    return attend(query, kv, w_out, conv_in, conv_gate, conv_taps, sb_bias, nz, nt)


def solution(mesh):
    torus = Mesh(
        mesh.devices.reshape(mesh.shape["sp"] // 8, 4, 2, mesh.shape["tp"]),
        ("sp_0", "sp_1", "sp_2", "tp"),
    )
    return jax.shard_map(
        local,
        mesh=torus,
        in_specs=(
            P(SP, "tp"),
            P(),
            P(SP, "tp"),
            P(SP, "tp"),
            P(SP, "tp"),
            P(SP, "tp"),
            P(SP, "tp"),
            P(None, "tp"),
            P("tp"),
            P("tp", SP),
            P("tp", SP),
        ),
        out_specs=(P(SP, "tp"), P("tp", SP)),
        check_vma=False,
    )
```

```python
import functools

import jax
import jax.numpy as jnp
from jax import lax
from jax.experimental import pallas as pl
from jax.experimental.pallas import tpu as pltpu
from jax.sharding import Mesh
from jax.sharding import PartitionSpec as P

HEAD = 64
SP = ("sp_0", "sp_1", "sp_2")
KEYS = 256
EPS = 1e-06
FLOOR = 0.02
LN2 = 0.6931471805599453
NT = (((1,), (1,)), ((), ()))
MESH = pl.DeviceIdType.MESH


class Spread:
    def __init__(self, nz, stride, own, buf, zs, zr, xs, xr, ps, pr):
        self.nz, self.own, self.buf = nz, own, buf
        self.zs, self.zr, self.xs, self.xr, self.ps, self.pr = zs, zr, xs, xr, ps, pr
        self.z, self.x, self.c = (lax.axis_index(a) for a in SP)
        self.ups, self.downs = nz // 2, (nz - 1) // 2
        self.stride = min(stride, self.ups)
        self.x_up, self.x_down = ({"sp_1": lax.rem(self.x + d, 4)} for d in (1, 3))
        self.partner = {"sp_2": 1 - self.c}
        on_z = [self.z_peer(up, r) for r in range(1, self.stride + 1) for up in (True, False)]
        self.peers = (*on_z, self.x_up, self.x_down, self.partner)

    def z_peer(self, up, r):
        return {"sp_0": lax.rem(self.z + r if up else self.z - r + self.nz, self.nz)}

    def limit(self, up):
        return self.ups if up else self.downs

    def plane(self, up, n):
        return lax.rem(self.z - n + self.nz, self.nz) if up else lax.rem(self.z + n, self.nz)

    def slot(self, up, n, dx=0):
        return self.buf.at[self.plane(up, n), lax.rem(self.x + dx, 4), self.c]

    def index(self, up, n):
        return n if up else self.ups + n

    def pass_on(self, up, n, src):
        for r in range(self.stride, 0, -1):
            k, slot = self.index(up, n + r), self.slot(up, n)
            sems = self.zs.at[k], self.zr.at[k]
            go = lambda r=r, sems=sems: remote(src, slot, *sems, self.z_peer(up, r)).start()
            when(n + r <= self.limit(up), go)

    def on_z(self, up, n):
        k, slot = self.index(up, n), self.slot(up, n)
        return remote(slot, slot, self.zs.at[k], self.zr.at[k], self.z_peer(up, 1))

    def along_x(self, up, n, way, src=None):
        k, slot = self.index(up, n), self.slot(up, n)
        peer = self.x_up if way == 0 else self.x_down
        return remote(slot if src is None else src, slot, self.xs.at[k, way], self.xr.at[k, way], peer)

    def far_x(self, up, n):
        k, slot = self.index(up, n), self.slot(up, n, 3 if up else 1)
        return remote(slot, slot, self.xs.at[k, 2], self.xr.at[k, 2], self.x_up if up else self.x_down)

    def across(self, up, n, core):
        k, row = self.index(up, n), self.buf.at[self.plane(up, n), :, core]
        return remote(row, row, self.ps.at[k], self.pr.at[k], self.partner)

    def each(self, n, work):
        when(n <= self.ups, lambda: work(True))
        when(n <= self.downs, lambda: work(False))

    def begin(self):
        own = self.own
        self.pass_on(True, 0, own)
        self.pass_on(False, 0, own)
        self.along_x(True, 0, 0, own).start()
        self.along_x(True, 0, 1, own).start()
        self.buf[self.z, self.x, self.c] = own[...]

    def step_z(self, n):
        def work(up):
            self.on_z(up, n).wait_recv()
            when(n % self.stride == 0, lambda: self.pass_on(up, n, self.slot(up, n)))
            for way in (0, 1):
                self.along_x(up, n, way).start()

        self.each(n, work)

    def step_x(self, n, first=False):
        def work(up):
            for way in (0, 1):
                self.along_x(up, n, way).wait_recv()
            self.far_x(up, n).start()

        work(True) if first else self.each(n, work)

    def step_far(self, n, first=False):
        def work(up):
            self.far_x(up, n).wait_recv()
            self.across(up, n, self.c).start()

        work(True) if first else self.each(n, work)

    def step_across(self, n, first=False):
        def work(up):
            self.across(up, n, 1 - self.c).wait_recv()

        work(True) if first else self.each(n, work)

    def finish(self):
        for k in range(self.nz):
            up = k <= self.ups
            n = k if up else k - self.ups
            if k:
                self.on_z(up, n).wait_send()
            for way in (0, 1):
                self.along_x(up, n, way).wait_send()
            self.far_x(up, n).wait_send()
            self.across(up, n, self.c).wait_send()


def remote(src, dst, ssem, rsem, peer):
    return pltpu.make_async_remote_copy(
        src_ref=src, dst_ref=dst, send_sem=ssem, recv_sem=rsem, device_id=peer, device_id_type=MESH
    )


def when(cond, work):
    if isinstance(cond, bool):
        if cond:
            work()
    else:
        pl.when(cond)(work)


def greet(peers):
    barrier = pltpu.get_barrier_semaphore()
    for peer in peers:
        pl.semaphore_signal(barrier, inc=1, device_id=peer, device_id_type=MESH)
    pl.semaphore_wait(barrier, len(peers))


def spread_sems(nz):
    dma = pltpu.SemaphoreType.DMA
    return [dma((nz,)), dma((nz,)), dma((nz, 3)), dma((nz, 3)), dma((nz,)), dma((nz,))]


def project_kernel(
    nz, nt, own_ref, stream_ref, gain_ref, out_rows_ref, kv_ref, q_ref, conv_ref, gate_ref,
    buf, heard, scaled, acc, zs, zr, xs, xr, ps, pr, ys, yr,
):
    net = Spread(nz, 4, own_ref, buf, zs, zr, xs, xr, ps, pr)
    y = lax.axis_index("tp")
    tokens = stream_ref.shape[0]
    others = [{"tp": lax.rem(y + r, nt)} for r in range(1, nt)]
    greet((*net.peers, *others))
    net.begin()
    sent = [
        remote(stream_ref, heard.at[y], ys.at[r], yr.at[r], others[r - 1]) for r in (2, 1, 3) if r < nt
    ]
    for one in sent:
        one.start()
    heard[y] = stream_ref[...]
    acc[...] = jnp.zeros_like(acc)
    share = nz // nt

    def scale():
        for r in range(1, nt):
            slot = heard.at[lax.rem(y + nt - r, nt)]
            remote(slot, slot, ys.at[r], yr.at[r], others[r - 1]).wait_recv()
        squares = jnp.zeros((tokens, 1), jnp.float32)
        for b in range(nt):
            piece = heard[b].astype(jnp.float32)
            squares = squares + jnp.sum(piece * piece, axis=1, keepdims=True)
            piece = (piece * gain_ref[b : b + 1, :]).astype(jnp.bfloat16)
            for j in range(share):
                scaled[b * share + j] = piece[:, 128 * j : 128 * (j + 1)]
        return squares

    def take(up, n):
        at = net.plane(up, n)
        rows = buf[at].reshape(128, acc.shape[1])
        acc[...] += jnp.dot(scaled[at], rows, preferred_element_type=jnp.float32)

    near = net.stride
    order = [0, *(q + r for q in range(0, net.ups, near) for r in range(near, 0, -1))]
    squares = None
    for i in range(len(order) + 6):
        if 0 < i < len(order):
            net.step_z(order[i])
        if 2 <= i < len(order) + 2:
            net.step_x(order[i - 2], i == 2)
        if 4 <= i < len(order) + 4:
            net.step_far(order[i - 4], i == 4)
        if 6 <= i:
            n = order[i - 6]
            if n == 0:
                squares = scale()
            net.step_across(n, n == 0)
            take(True, n)
            if 0 < n <= net.downs:
                take(False, n)
    row_scale = lax.rsqrt(squares / (nz * 128) + EPS)
    mine = (acc[...] * row_scale).astype(jnp.bfloat16)
    wide = conv_ref.shape[1]
    heads = wide // HEAD
    kv_ref[pl.ds(0, tokens), :] = mine[:, : 2 * HEAD]
    kv_ref[pl.ds(tokens, 64), :] = out_rows_ref[...]
    for h in range(heads):
        begin = 2 * HEAD + h * HEAD
        q = mine[:, begin : begin + HEAD].astype(jnp.float32) * (HEAD ** (-0.5) / LN2)
        high = q.astype(jnp.bfloat16).astype(jnp.float32)
        q_ref[pl.ds(h * tokens, tokens), :] = jnp.concatenate([high, q - high], axis=1).astype(jnp.bfloat16)
    conv_ref[...] = mine[:, 2 * HEAD + wide : 2 * HEAD + 2 * wide]
    gate_ref[...] = mine[:, 2 * HEAD + 2 * wide :]
    for one in sent:
        one.wait_send()
    net.finish()


def project(rows, stream, norm_gain, w_out, nz, nt):
    tokens = stream.shape[0]
    wide = (rows.shape[1] - 2 * HEAD) // 3
    cols = w_out.shape[0] // 4
    out_rows = w_out.reshape(4, cols, 16).transpose(0, 2, 1).reshape(64, cols)
    vmem = pl.BlockSpec(memory_space=pltpu.VMEM)
    dma = pltpu.SemaphoreType.DMA
    shapes = [(tokens + 64, 2 * HEAD), (wide // HEAD * tokens, 2 * HEAD), (tokens, wide), (tokens, wide)]
    return pl.pallas_call(
        functools.partial(project_kernel, nz, nt),
        name="project",
        out_shape=[jax.ShapeDtypeStruct(s, jnp.bfloat16) for s in shapes],
        in_specs=[vmem] * 4,
        out_specs=[vmem] * 4,
        scratch_shapes=[
            pltpu.VMEM((nz, 4, 2, *rows.shape), jnp.bfloat16),
            pltpu.VMEM((nt, *stream.shape), jnp.bfloat16),
            pltpu.VMEM((nz, tokens, 128), jnp.bfloat16),
            pltpu.VMEM((tokens, rows.shape[1]), jnp.float32),
            *spread_sems(nz),
            dma((nt,)),
            dma((nt,)),
        ],
        compiler_params=pltpu.CompilerParams(collective_id=0, has_side_effects=True),
    )(rows, stream, norm_gain.reshape(nt, -1), out_rows)


def attend_kernel(
    nz, nt, bias_ref, q_ref, own_ref, conv_ref, gate_ref, taps_ref, tri_ref, mixed_ref, weight_ref,
    buf, halo, o_new, s_new, o_old, s_old, part, heard, zs, zr, xs, xr, ps, pr, hs, hr, ys, yr,
):
    net = Spread(nz, 2, own_ref, buf, zs, zr, xs, xr, ps, pr)
    me = (net.z * 4 + net.x) * 2 + net.c
    y = lax.axis_index("tp")
    heads = bias_ref.shape[0]
    rows = q_ref.shape[0] // heads
    total = nz * 8

    def device(index):
        return {"sp_0": lax.div(index, 8), "sp_1": lax.rem(lax.div(index, 2), 4), "sp_2": lax.rem(index, 2)}

    ahead, behind = device(lax.rem(me + 1, total)), device(lax.rem(me + total - 1, total))
    others = [{"tp": lax.rem(y + r, nt)} for r in range(1, nt)]
    greet((*net.peers, ahead, behind, *others))
    net.begin()
    tail = remote(conv_ref.at[pl.ds(rows - 16, 16), :], halo, hs, hr, ahead)
    tail.start()
    for ref in (o_new, s_new, o_old, s_old):
        ref[...] = jnp.zeros_like(ref)

    def sweep(at, masked):
        out, gone = None, None
        for i in (3, 2, 1, 0):
            kv = buf[at, i, :, pl.ds(0, rows), :].reshape(KEYS, 2 * HEAD)
            both = jnp.concatenate([kv[:, :HEAD], kv[:, :HEAD]], axis=1)
            score = lax.dot_general(q_ref[...], both, NT, preferred_element_type=jnp.float32)
            score = jnp.concatenate(
                [score[h * rows : (h + 1) * rows] + bias_ref[h] for h in range(heads)], axis=0
            )
            if masked:
                key_pos = i * KEYS + lax.broadcasted_iota(jnp.int32, score.shape, 1)
                query_pos = lax.rem(me, 8) * rows + lax.rem(
                    lax.broadcasted_iota(jnp.int32, score.shape, 0), rows
                )
                score = jnp.where(key_pos < query_pos, score, -1e30)
            fail = jnp.maximum(score, lax.log2(1.0 + jnp.exp2(jnp.minimum(score, 80.0))))
            later = jnp.dot(fail.astype(jnp.bfloat16), tri_ref[...], preferred_element_type=jnp.float32)
            power = (score - fail) - later
            block = later[:, :1] + fail[:, :1]
            if gone is None:
                gone = jnp.broadcast_to(block, (heads * rows, 2 * HEAD))
            else:
                power = power - jnp.concatenate([gone, gone], axis=1)
                gone = gone + block
            stick = jnp.exp2(power).astype(jnp.bfloat16)
            term = jnp.dot(stick, kv, preferred_element_type=jnp.float32)
            out = term if out is None else out + term
        return out, gone

    def take_new(n, masked=False):
        out, gone = sweep(net.plane(True, n), masked)
        before = s_new[...]
        o_new[...] += jnp.exp2(-before) * out
        s_new[...] = before + gone

    def take_old(n):
        out, gone = sweep(net.plane(False, n), False)
        o_old[...] = o_old[...] * jnp.exp2(-gone) + out
        s_old[...] += gone

    net.step_x(0, True)
    net.step_z(1)
    net.step_z(2)
    net.step_far(0, True)
    net.step_x(1)
    net.step_z(3)
    net.step_z(4)
    net.step_across(0, True)
    take_new(0, True)
    net.step_x(2)
    net.step_far(1)
    net.step_x(3)

    @pl.loop(1, net.ups + 1)
    def _(n):
        net.step_z(n + 4)
        net.step_across(n)
        pl.when(net.z - n >= 0)(lambda: take_new(n))
        net.step_far(n + 1)
        net.step_x(n + 3)
        pl.when((net.z + n >= nz) & (n <= net.downs))(lambda: take_old(n))

    gone = s_new[...]
    out = o_new[...] + jnp.exp2(-gone) * o_old[...]
    survived = (gone + s_old[...]) * LN2
    weight = jnp.log(jnp.maximum(1.0 - jnp.exp(-survived), FLOOR))
    diagonal = lax.broadcasted_iota(jnp.int32, (rows, rows), 0) == lax.broadcasted_iota(
        jnp.int32, (rows, rows), 1
    )
    for h in range(heads):
        weight_ref[pl.ds(h, 1), :] = jnp.sum(
            jnp.where(diagonal, weight[h * rows : (h + 1) * rows], 0.0), axis=0, keepdims=True
        )
    attended = [out[h * rows : (h + 1) * rows, HEAD:] for h in range(heads)]

    tail.wait_recv()
    now = conv_ref[...].astype(jnp.float32)
    last = halo[...].astype(jnp.float32) * jnp.where(me > 0, 1.0, 0.0)
    row = lax.broadcasted_iota(jnp.int32, now.shape, 0)
    one = jnp.where(row == 0, last[15:16], pltpu.roll(now, 1, 0))
    two = jnp.where(row == 0, last[14:15], jnp.where(row == 1, last[15:16], pltpu.roll(now, 2, 0)))
    conv = taps_ref[0:1, :] * two + taps_ref[1:2, :] * one + taps_ref[2:3, :] * now
    conv = gate_ref[...].astype(jnp.float32) * conv
    act = jnp.concatenate([*attended, conv], axis=1).astype(jnp.bfloat16)

    share = nz // nt

    def project(to):
        planes = pl.ds(to * share, share)
        acc = None
        for j in range(4):
            w = buf[planes, :, :, pl.ds(rows + 16 * j, 16), :].reshape(share * 128, 128)
            term = lax.dot_general(
                act[:, 128 * j : 128 * (j + 1)], w, NT, preferred_element_type=jnp.float32
            )
            acc = term if acc is None else acc + term
        return acc.astype(jnp.bfloat16)

    sent = []
    for r in [*range(2, nt), 1] if nt > 1 else []:
        part[r] = project(lax.rem(y + r, nt))
        sent.append(remote(part.at[r], heard.at[r], ys.at[r], yr.at[r], others[r - 1]))
        sent[-1].start()
    mixed = project(y).astype(jnp.float32)
    for one_sent in sent:
        one_sent.wait_recv()
    for r in range(1, nt):
        mixed = mixed + heard[r].astype(jnp.float32)
    mixed_ref[...] = mixed.astype(jnp.bfloat16)
    for one_sent in sent:
        one_sent.wait_send()
    tail.wait_send()
    net.finish()


def attend(own, q, conv_in, conv_gate, conv_taps, sb_bias, nz, nt):
    tokens = conv_in.shape[0]
    heads = q.shape[0] // tokens
    order = jnp.arange(KEYS)
    tri = (order[:, None] > order[None, :]).astype(jnp.bfloat16)
    vmem = pl.BlockSpec(memory_space=pltpu.VMEM)
    out_cols = nz * 128 // nt
    wide = pltpu.VMEM((heads * tokens, 2 * HEAD), jnp.float32)
    parts = pltpu.VMEM((nt, tokens, out_cols), jnp.bfloat16)
    dma = pltpu.SemaphoreType.DMA
    return pl.pallas_call(
        functools.partial(attend_kernel, nz, nt),
        name="attend",
        out_shape=(
            jax.ShapeDtypeStruct((tokens, out_cols), jnp.bfloat16),
            jax.ShapeDtypeStruct((heads, tokens), jnp.float32),
        ),
        in_specs=[pl.BlockSpec(memory_space=pltpu.SMEM)] + [vmem] * 6,
        out_specs=(vmem, vmem),
        scratch_shapes=[
            pltpu.VMEM((nz, 4, 2, *own.shape), jnp.bfloat16),
            pltpu.VMEM((16, conv_in.shape[1]), jnp.bfloat16),
            *[wide] * 4,
            *[parts] * 2,
            *spread_sems(nz),
            dma,
            dma,
            dma((nt,)),
            dma((nt,)),
        ],
        compiler_params=pltpu.CompilerParams(collective_id=1, has_side_effects=True),
    )(sb_bias / LN2, q, own, conv_in, conv_gate, conv_taps, tri)


def local(
    stream,
    norm_gain,
    w_query,
    w_key,
    w_value,
    w_conv_in,
    w_conv_gate,
    conv_taps,
    sb_bias,
    w_out_attn,
    w_out_conv,
):
    nz, nt = lax.axis_size(SP[0]), lax.axis_size("tp")
    rows = jnp.concatenate([w_key, w_value, w_query, w_conv_in, w_conv_gate], axis=1)
    w_out = jnp.concatenate([w_out_attn, w_out_conv], axis=0)
    own, q, conv_in, conv_gate = project(rows, stream, norm_gain, w_out, nz, nt)
    return attend(own, q, conv_in, conv_gate, conv_taps, sb_bias, nz, nt)


def solution(mesh):
    torus = Mesh(
        mesh.devices.reshape(mesh.shape["sp"] // 8, 4, 2, mesh.shape["tp"]),
        ("sp_0", "sp_1", "sp_2", "tp"),
    )
    return jax.shard_map(
        local,
        mesh=torus,
        in_specs=(
            P(SP, "tp"),
            P(),
            P(SP, "tp"),
            P(SP, "tp"),
            P(SP, "tp"),
            P(SP, "tp"),
            P(SP, "tp"),
            P(None, "tp"),
            P("tp"),
            P("tp", SP),
            P("tp", SP),
        ),
        out_specs=(P(SP, "tp"), P("tp", SP)),
        check_vma=False,
    )
```

```python
import functools

import jax
import jax.numpy as jnp
from jax import lax
from jax.experimental import pallas as pl
from jax.experimental.pallas import tpu as pltpu
from jax.sharding import Mesh
from jax.sharding import PartitionSpec as P

HEAD = 64
SP = ("sp_0", "sp_1", "sp_2")
KEYS = 256
EPS = 1e-06
FLOOR = 0.02
LN2 = 0.6931471805599453
NT = (((1,), (1,)), ((), ()))
MESH = pl.DeviceIdType.MESH


PROJECT_ORDER = (
    "x0", "z3", "z1", "z2", "f0", "p0", "x3", "x1", "z6", "z4", "x2", "z5",
    "f3", "f1", "p3", "x6", "p1", "z7", "z8", "x4", "f2", "x5", "p2", "f6",
    "x7", "p6", "x8", "f4", "f5", "p4", "p5", "f7", "f8", "p7", "p8",
)
ATTEND_ORDER = (
    ("z1", "x0", "z2", "x1", "f0", "z3", "p0",),
    ("x2", "f1", "z4", "p1",),
    ("x3",),
    ("z5", "f2", "x4", "z6", "p2",),
    ("f3",),
    ("x5", "p3", "z7",),
    ("f4",),
    ("z8", "x6", "p4", "f5",),
    (),
    ("x7", "p5",),
    ("x8", "f6",),
    ("p6",),
    ("f7",),
    ("f8", "p7",),
    ("p8",),
    (),
)


def order_of(nz, table):
    if nz == 16:
        return table
    ups, downs, waits = nz // 2, (nz - 1) // 2, [("x0", "f0", "p0")]
    for n in range(1, ups + 1):
        waits += [tuple(kind + str(n) for kind in "zxfp"), *[()] * (n <= downs)]
    return waits


class Spread:
    def __init__(self, nz, stride, far_first, own, buf, zs, zr, xs, xr, ps, pr):
        self.nz, self.own, self.buf = nz, own, buf
        self.zs, self.zr, self.xs, self.xr, self.ps, self.pr = zs, zr, xs, xr, ps, pr
        self.z, self.x, self.c = (lax.axis_index(a) for a in SP)
        self.ups, self.downs = nz // 2, (nz - 1) // 2
        self.stride = min(stride, self.ups)
        self.reach = [*range(1, self.stride + 1)][:: -1 if far_first else 1]
        self.x_up, self.x_down = ({"sp_1": lax.rem(self.x + d, 4)} for d in (1, 3))
        self.partner = {"sp_2": 1 - self.c}
        on_z = [self.z_peer(up, r) for r in range(1, self.stride + 1) for up in (True, False)]
        self.peers = (*on_z, self.x_up, self.x_down, self.partner)

    def z_peer(self, up, r):
        return {"sp_0": lax.rem(self.z + r if up else self.z - r + self.nz, self.nz)}

    def limit(self, up):
        return self.ups if up else self.downs

    def plane(self, up, n):
        return lax.rem(self.z - n + self.nz, self.nz) if up else lax.rem(self.z + n, self.nz)

    def slot(self, up, n, dx=0):
        return self.buf.at[self.plane(up, n), lax.rem(self.x + dx, 4), self.c]

    def index(self, up, n):
        return n if up else self.ups + n

    def pass_on(self, up, n, src):
        for r in self.reach:
            k, slot = self.index(up, n + r), self.slot(up, n)
            sems = self.zs.at[k], self.zr.at[k]
            go = lambda r=r, sems=sems: remote(src, slot, *sems, self.z_peer(up, r)).start()
            when(n + r <= self.limit(up), go)

    def on_z(self, up, n):
        k, slot = self.index(up, n), self.slot(up, n)
        return remote(slot, slot, self.zs.at[k], self.zr.at[k], self.z_peer(up, 1))

    def along_x(self, up, n, way, src=None):
        k, slot = self.index(up, n), self.slot(up, n)
        peer = self.x_up if way == 0 else self.x_down
        return remote(slot if src is None else src, slot, self.xs.at[k, way], self.xr.at[k, way], peer)

    def far_x(self, up, n):
        k, slot = self.index(up, n), self.slot(up, n, 3 if up else 1)
        return remote(slot, slot, self.xs.at[k, 2], self.xr.at[k, 2], self.x_up if up else self.x_down)

    def across(self, up, n, core):
        k, row = self.index(up, n), self.buf.at[self.plane(up, n), :, core]
        return remote(row, row, self.ps.at[k], self.pr.at[k], self.partner)

    def each(self, n, work):
        when(n <= self.ups, lambda: work(True))
        when(n <= self.downs, lambda: work(False))

    def begin(self):
        own = self.own
        self.pass_on(True, 0, own)
        self.pass_on(False, 0, own)
        self.along_x(True, 0, 0, own).start()
        self.along_x(True, 0, 1, own).start()
        self.buf[self.z, self.x, self.c] = own[...]

    def step_z(self, n):
        def work(up):
            self.on_z(up, n).wait_recv()
            when(n % self.stride == 0, lambda: self.pass_on(up, n, self.slot(up, n)))
            for way in (0, 1):
                self.along_x(up, n, way).start()

        self.each(n, work)

    def step_x(self, n, first=False):
        def work(up):
            for way in (0, 1):
                self.along_x(up, n, way).wait_recv()
            self.far_x(up, n).start()

        work(True) if first else self.each(n, work)

    def step_far(self, n, first=False):
        def work(up):
            self.far_x(up, n).wait_recv()
            self.across(up, n, self.c).start()

        work(True) if first else self.each(n, work)

    def step_across(self, n, first=False):
        def work(up):
            self.across(up, n, 1 - self.c).wait_recv()

        work(True) if first else self.each(n, work)

    def run(self, waits):
        steps = {"z": self.step_z, "x": self.step_x, "f": self.step_far, "p": self.step_across}
        for one in waits:
            n = int(one[1:])
            steps[one[0]](n, *([] if n else [True]))

    def finish(self):
        for k in range(self.nz):
            up = k <= self.ups
            n = k if up else k - self.ups
            if k:
                self.on_z(up, n).wait_send()
            for way in (0, 1):
                self.along_x(up, n, way).wait_send()
            self.far_x(up, n).wait_send()
            self.across(up, n, self.c).wait_send()


def remote(src, dst, ssem, rsem, peer):
    return pltpu.make_async_remote_copy(
        src_ref=src, dst_ref=dst, send_sem=ssem, recv_sem=rsem, device_id=peer, device_id_type=MESH
    )


def when(cond, work):
    if isinstance(cond, bool):
        if cond:
            work()
    else:
        pl.when(cond)(work)


def greet(peers):
    barrier = pltpu.get_barrier_semaphore()
    for peer in peers:
        pl.semaphore_signal(barrier, inc=1, device_id=peer, device_id_type=MESH)
    pl.semaphore_wait(barrier, len(peers))


def spread_sems(nz):
    dma = pltpu.SemaphoreType.DMA
    return [dma((nz,)), dma((nz,)), dma((nz, 3)), dma((nz, 3)), dma((nz,)), dma((nz,))]


def project_kernel(
    nz, nt, own_ref, stream_ref, gain_ref, attn_ref, convw_ref, kv_ref, q_ref, conv_ref, gate_ref,
    buf, heard, scaled, acc, zs, zr, xs, xr, ps, pr, ys, yr,
):
    net = Spread(nz, 3, True, own_ref, buf, zs, zr, xs, xr, ps, pr)
    y = lax.axis_index("tp")
    tokens = stream_ref.shape[0]
    others = [{"tp": lax.rem(y + r, nt)} for r in range(1, nt)]
    greet((*net.peers, *others))
    net.begin()
    sent = [
        remote(stream_ref, heard.at[y], ys.at[r], yr.at[r], others[r - 1]) for r in (2, 1, 3) if r < nt
    ]
    for one in sent:
        one.start()
    heard[y] = stream_ref[...]
    acc[...] = jnp.zeros_like(acc)
    share = nz // nt

    def scale():
        for r in range(1, nt):
            slot = heard.at[lax.rem(y + nt - r, nt)]
            remote(slot, slot, ys.at[r], yr.at[r], others[r - 1]).wait_recv()
        squares = jnp.zeros((tokens, 1), jnp.float32)
        for b in range(nt):
            piece = heard[b].astype(jnp.float32)
            squares = squares + jnp.sum(piece * piece, axis=1, keepdims=True)
            piece = (piece * gain_ref[:, b * share * 128 : (b + 1) * share * 128]).astype(jnp.bfloat16)
            for j in range(share):
                scaled[b * share + j] = piece[:, 128 * j : 128 * (j + 1)]
        return squares

    def take(up, n):
        at = net.plane(up, n)
        rows = buf[at].reshape(128, acc.shape[1])
        acc[...] += jnp.dot(scaled[at], rows, preferred_element_type=jnp.float32)

    for j in range(4):
        source = (attn_ref, convw_ref)[j // 2]
        kv_ref[pl.ds(tokens + 16 * j, 16), :] = source[:, 128 * (j % 2) : 128 * (j % 2 + 1)]

    squares = None
    waits = PROJECT_ORDER if nz == 16 else [one for some in order_of(nz, None) for one in some]
    for one in waits:
        net.run([one])
        if one[0] == "p":
            n = int(one[1:])
            if n == 0:
                squares = scale()
            take(True, n)
            if 0 < n <= net.downs:
                take(False, n)
    row_scale = lax.rsqrt(squares / (nz * 128) + EPS)
    mine = (acc[...] * row_scale).astype(jnp.bfloat16)
    wide = conv_ref.shape[1]
    heads = wide // HEAD
    kv_ref[pl.ds(0, tokens), :] = mine[:, : 2 * HEAD]
    for h in range(heads):
        begin = 2 * HEAD + h * HEAD
        q = mine[:, begin : begin + HEAD].astype(jnp.float32) * (HEAD ** (-0.5) / LN2)
        high = q.astype(jnp.bfloat16).astype(jnp.float32)
        q_ref[pl.ds(h * tokens, tokens), :] = jnp.concatenate([high, q - high], axis=1).astype(jnp.bfloat16)
    conv_ref[...] = mine[:, 2 * HEAD + wide : 2 * HEAD + 2 * wide]
    gate_ref[...] = mine[:, 2 * HEAD + 2 * wide :]
    for one in sent:
        one.wait_send()
    net.finish()


def project(rows, stream, norm_gain, w_out_attn, w_out_conv, nz, nt):
    tokens = stream.shape[0]
    wide = (rows.shape[1] - 2 * HEAD) // 3
    vmem = pl.BlockSpec(memory_space=pltpu.VMEM)
    dma = pltpu.SemaphoreType.DMA
    shapes = [(tokens + 64, 2 * HEAD), (wide // HEAD * tokens, 2 * HEAD), (tokens, wide), (tokens, wide)]
    return pl.pallas_call(
        functools.partial(project_kernel, nz, nt),
        name="project",
        out_shape=[jax.ShapeDtypeStruct(s, jnp.bfloat16) for s in shapes],
        in_specs=[vmem] * 5,
        out_specs=[vmem] * 4,
        scratch_shapes=[
            pltpu.VMEM((nz, 4, 2, *rows.shape), jnp.bfloat16),
            pltpu.VMEM((nt, *stream.shape), jnp.bfloat16),
            pltpu.VMEM((nz, tokens, 128), jnp.bfloat16),
            pltpu.VMEM((tokens, rows.shape[1]), jnp.float32),
            *spread_sems(nz),
            dma((nt,)),
            dma((nt,)),
        ],
        compiler_params=pltpu.CompilerParams(collective_id=0, has_side_effects=True),
    )(rows, stream, norm_gain[None, :], w_out_attn.T, w_out_conv.T)


def attend_kernel(
    nz, nt, bias_ref, q_ref, own_ref, conv_ref, gate_ref, taps_ref, mixed_ref, weight_ref,
    buf, tri, halo, o_new, s_new, o_old, s_old, part, heard, zs, zr, xs, xr, ps, pr, hs, hr, ys, yr,
):
    net = Spread(nz, 2, False, own_ref, buf, zs, zr, xs, xr, ps, pr)
    me = (net.z * 4 + net.x) * 2 + net.c
    y = lax.axis_index("tp")
    heads = bias_ref.shape[0]
    rows = q_ref.shape[0] // heads
    total = nz * 8

    def device(index):
        return {"sp_0": lax.div(index, 8), "sp_1": lax.rem(lax.div(index, 2), 4), "sp_2": lax.rem(index, 2)}

    ahead, behind = device(lax.rem(me + 1, total)), device(lax.rem(me + total - 1, total))
    others = [{"tp": lax.rem(y + r, nt)} for r in range(1, nt)]
    greet((*net.peers, ahead, behind, *others))
    net.begin()
    tail = remote(conv_ref.at[pl.ds(rows - 16, 16), :], halo, hs, hr, ahead)
    tail.start()
    after = lax.broadcasted_iota(jnp.int32, tri.shape, 0) > lax.broadcasted_iota(jnp.int32, tri.shape, 1)
    tri[...] = jnp.where(after, 1.0, 0.0).astype(jnp.bfloat16)
    for ref in (o_new, s_new, o_old, s_old):
        ref[...] = jnp.zeros_like(ref)

    def sweep(at, masked):
        out, gone = None, None
        for i in (3, 2, 1, 0):
            kv = buf[at, i, :, pl.ds(0, rows), :].reshape(KEYS, 2 * HEAD)
            both = jnp.concatenate([kv[:, :HEAD], kv[:, :HEAD]], axis=1)
            score = lax.dot_general(q_ref[...], both, NT, preferred_element_type=jnp.float32)
            score = jnp.concatenate(
                [score[h * rows : (h + 1) * rows] + bias_ref[h] / LN2 for h in range(heads)], axis=0
            )
            if masked:
                key_pos = i * KEYS + lax.broadcasted_iota(jnp.int32, score.shape, 1)
                query_pos = lax.rem(me, 8) * rows + lax.rem(
                    lax.broadcasted_iota(jnp.int32, score.shape, 0), rows
                )
                score = jnp.where(key_pos < query_pos, score, -1e30)
            fail = jnp.maximum(score, lax.log2(1.0 + jnp.exp2(jnp.minimum(score, 80.0))))
            later = jnp.dot(fail.astype(jnp.bfloat16), tri[...], preferred_element_type=jnp.float32)
            power = (score - fail) - later
            block = later[:, :1] + fail[:, :1]
            if gone is None:
                gone = jnp.broadcast_to(block, (heads * rows, 2 * HEAD))
            else:
                power = power - jnp.concatenate([gone, gone], axis=1)
                gone = gone + block
            stick = jnp.exp2(power).astype(jnp.bfloat16)
            term = jnp.dot(stick, kv, preferred_element_type=jnp.float32)
            out = term if out is None else out + term
        return out, gone

    def take_new(n, masked=False):
        out, gone = sweep(net.plane(True, n), masked)
        before = s_new[...]
        o_new[...] += jnp.exp2(-before) * out
        s_new[...] = before + gone

    def take_old(n):
        out, gone = sweep(net.plane(False, n), False)
        o_old[...] = o_old[...] * jnp.exp2(-gone) + out
        s_old[...] += gone

    waits = order_of(nz, ATTEND_ORDER)
    net.run(waits[0])
    take_new(0, True)

    def at_step(n, offset):
        for i in range(1, net.ups + 1):
            if 2 * i - 1 + offset < len(waits) and waits[2 * i - 1 + offset]:
                pl.when(n == i)(functools.partial(net.run, waits[2 * i - 1 + offset]))

    @pl.loop(1, net.ups + 1)
    def _(n):
        at_step(n, 0)
        pl.when(net.z - n >= 0)(lambda: take_new(n))
        at_step(n, 1)
        pl.when((net.z + n >= nz) & (n <= net.downs))(lambda: take_old(n))

    gone = s_new[...]
    out = o_new[...] + jnp.exp2(-gone) * o_old[...]
    survived = (gone + s_old[...]) * LN2
    weight = jnp.log(jnp.maximum(1.0 - jnp.exp(-survived), FLOOR))
    diagonal = lax.broadcasted_iota(jnp.int32, (rows, rows), 0) == lax.broadcasted_iota(
        jnp.int32, (rows, rows), 1
    )
    for h in range(heads):
        weight_ref[pl.ds(h, 1), :] = jnp.sum(
            jnp.where(diagonal, weight[h * rows : (h + 1) * rows], 0.0), axis=0, keepdims=True
        )
    attended = [out[h * rows : (h + 1) * rows, HEAD:] for h in range(heads)]

    tail.wait_recv()
    now = conv_ref[...].astype(jnp.float32)
    last = halo[...].astype(jnp.float32) * jnp.where(me > 0, 1.0, 0.0)
    row = lax.broadcasted_iota(jnp.int32, now.shape, 0)
    one = jnp.where(row == 0, last[15:16], pltpu.roll(now, 1, 0))
    two = jnp.where(row == 0, last[14:15], jnp.where(row == 1, last[15:16], pltpu.roll(now, 2, 0)))
    conv = taps_ref[0:1, :] * two + taps_ref[1:2, :] * one + taps_ref[2:3, :] * now
    conv = gate_ref[...].astype(jnp.float32) * conv
    act = jnp.concatenate([*attended, conv], axis=1).astype(jnp.bfloat16)

    share = nz // nt

    def project(to):
        planes = pl.ds(to * share, share)
        acc = None
        for j in range(4):
            w = buf[planes, :, :, pl.ds(rows + 16 * j, 16), :].reshape(share * 128, 128)
            term = lax.dot_general(
                act[:, 128 * j : 128 * (j + 1)], w, NT, preferred_element_type=jnp.float32
            )
            acc = term if acc is None else acc + term
        return acc.astype(jnp.bfloat16)

    sent = []
    for r in [*range(2, nt), 1] if nt > 1 else []:
        part[r] = project(lax.rem(y + r, nt))
        sent.append(remote(part.at[r], heard.at[r], ys.at[r], yr.at[r], others[r - 1]))
        sent[-1].start()
    mixed = project(y).astype(jnp.float32)
    for one_sent in sent:
        one_sent.wait_recv()
    for r in range(1, nt):
        mixed = mixed + heard[r].astype(jnp.float32)
    mixed_ref[...] = mixed.astype(jnp.bfloat16)
    for one_sent in sent:
        one_sent.wait_send()
    tail.wait_send()
    net.finish()


def attend(own, q, conv_in, conv_gate, conv_taps, sb_bias, nz, nt):
    tokens = conv_in.shape[0]
    heads = q.shape[0] // tokens
    vmem = pl.BlockSpec(memory_space=pltpu.VMEM)
    out_cols = nz * 128 // nt
    wide = pltpu.VMEM((heads * tokens, 2 * HEAD), jnp.float32)
    parts = pltpu.VMEM((nt, tokens, out_cols), jnp.bfloat16)
    dma = pltpu.SemaphoreType.DMA
    return pl.pallas_call(
        functools.partial(attend_kernel, nz, nt),
        name="attend",
        out_shape=(
            jax.ShapeDtypeStruct((tokens, out_cols), jnp.bfloat16),
            jax.ShapeDtypeStruct((heads, tokens), jnp.float32),
        ),
        in_specs=[pl.BlockSpec(memory_space=pltpu.SMEM)] + [vmem] * 5,
        out_specs=(vmem, vmem),
        scratch_shapes=[
            pltpu.VMEM((nz, 4, 2, *own.shape), jnp.bfloat16),
            pltpu.VMEM((KEYS, KEYS), jnp.bfloat16),
            pltpu.VMEM((16, conv_in.shape[1]), jnp.bfloat16),
            *[wide] * 4,
            *[parts] * 2,
            *spread_sems(nz),
            dma,
            dma,
            dma((nt,)),
            dma((nt,)),
        ],
        compiler_params=pltpu.CompilerParams(collective_id=1, has_side_effects=True),
    )(sb_bias, q, own, conv_in, conv_gate, conv_taps)


def local(
    stream,
    norm_gain,
    w_query,
    w_key,
    w_value,
    w_conv_in,
    w_conv_gate,
    conv_taps,
    sb_bias,
    w_out_attn,
    w_out_conv,
):
    nz, nt = lax.axis_size(SP[0]), lax.axis_size("tp")
    rows = jnp.concatenate([w_key, w_value, w_query, w_conv_in, w_conv_gate], axis=1)
    own, q, conv_in, conv_gate = project(rows, stream, norm_gain, w_out_attn, w_out_conv, nz, nt)
    return attend(own, q, conv_in, conv_gate, conv_taps, sb_bias, nz, nt)


def solution(mesh):
    torus = Mesh(
        mesh.devices.reshape(mesh.shape["sp"] // 8, 4, 2, mesh.shape["tp"]),
        ("sp_0", "sp_1", "sp_2", "tp"),
    )
    return jax.shard_map(
        local,
        mesh=torus,
        in_specs=(
            P(SP, "tp"),
            P(),
            P(SP, "tp"),
            P(SP, "tp"),
            P(SP, "tp"),
            P(SP, "tp"),
            P(SP, "tp"),
            P(None, "tp"),
            P("tp"),
            P("tp", SP),
            P("tp", SP),
        ),
        out_specs=(P(SP, "tp"), P("tp", SP)),
        check_vma=False,
    )
```

```python
import functools

import jax
import jax.numpy as jnp
from jax import lax
from jax.experimental import pallas as pl
from jax.experimental.pallas import tpu as pltpu
from jax.sharding import Mesh
from jax.sharding import PartitionSpec as P

HEAD = 64
SP = ("sp_0", "sp_1", "sp_2")
KEYS = 256
EPS = 1e-06
FLOOR = 0.02
LN2 = 0.6931471805599453
NT = (((1,), (1,)), ((), ()))
MESH = pl.DeviceIdType.MESH


PROJECT_ORDER = (
    "ix0", "iz3", "iz1", "iz2", "if0", "ip0", "ix3", "ix1", "iz6", "iz4", "ix2", "iz5",
    "if3", "if1", "ip3", "ix6", "ip1", "iz7", "iz8", "wb0", "ix4", "if2", "ix5", "ip2",
    "if6", "wz1", "ix7", "ip6", "ix8", "wx0", "if4", "if5", "wz2", "wx1", "ip4", "if7",
    "ip5", "if8", "wf0", "ip7", "wz3", "ip8",
)
ATTEND_ORDER = (
    ("wx2", "wf1", "wp0", "wp1", "wz4", "wx3", "kz1", "kx0", "wf2", "wx4", "wz5", "wp2", "wf3", "kz2", "wp3", "kx1", "kf0", "wz6", "wf4", "kz3", "wx5", "kp0",),
    ("kz4", "kx2", "kf1", "wz7", "wp4", "wx6", "kp1",),
    ("kx3", "wf5",),
    ("kz5", "kx4", "kf2", "wp5", "wz8", "wx7", "kz6", "wf6", "kp2",),
    ("kf3", "wp6",),
    ("kz7", "kx5", "kf4", "kp3",),
    ("kz8", "wx8", "kp4", "wf7",),
    ("kx6", "wp7",),
    ("kx7", "kf5",),
    ("kx8", "wf8", "kp5",),
    ("kf6", "wp8",),
    ("kf7", "kp6",),
    ("kf8", "kp7",),
    ("kp8",),
    (),
    (),
)
LAST_ORDER = ()


def orders_of(nz):
    if nz == 16:
        return PROJECT_ORDER, ATTEND_ORDER, LAST_ORDER
    ups, downs = nz // 2, (nz - 1) // 2
    first = lambda s: [s + kind + "0" for kind in "xfp"]
    waits = lambda s, n: [s + kind + str(n) for kind in "zxfp"]
    rows = [*first("i"), *(one for n in range(1, ups + 1) for one in waits("i", n))]
    keys = [first("k")]
    for n in range(1, ups + 1):
        keys += [waits("k", n), *[[]] * (n <= downs)]
    last = ["wb0", *first("w"), *(one for n in range(1, ups + 1) for one in waits("w", n))]
    return rows, keys, last


class Spread:
    def __init__(self, nz, stride, far_first, own, buf, zs, zr, xs, xr, ps, pr):
        self.nz, self.own, self.buf = nz, own, buf
        self.zs, self.zr, self.xs, self.xr, self.ps, self.pr = zs, zr, xs, xr, ps, pr
        self.z, self.x, self.c = (lax.axis_index(a) for a in SP)
        self.ups, self.downs = nz // 2, (nz - 1) // 2
        self.stride = min(stride, self.ups)
        self.reach = [*range(1, self.stride + 1)][:: -1 if far_first else 1]
        self.x_up, self.x_down = ({"sp_1": lax.rem(self.x + d, 4)} for d in (1, 3))
        self.partner = {"sp_2": 1 - self.c}
        on_z = [self.z_peer(up, r) for r in range(1, self.stride + 1) for up in (True, False)]
        self.peers = (*on_z, self.x_up, self.x_down, self.partner)

    def z_peer(self, up, r):
        return {"sp_0": lax.rem(self.z + r if up else self.z - r + self.nz, self.nz)}

    def limit(self, up):
        return self.ups if up else self.downs

    def plane(self, up, n):
        return lax.rem(self.z - n + self.nz, self.nz) if up else lax.rem(self.z + n, self.nz)

    def slot(self, up, n, dx=0):
        return self.buf.at[self.plane(up, n), lax.rem(self.x + dx, 4), self.c]

    def index(self, up, n):
        return n if up else self.ups + n

    def pass_on(self, up, n, src):
        for r in self.reach:
            k, slot = self.index(up, n + r), self.slot(up, n)
            sems = self.zs.at[k], self.zr.at[k]
            go = lambda r=r, sems=sems: remote(src, slot, *sems, self.z_peer(up, r)).start()
            when(n + r <= self.limit(up), go)

    def on_z(self, up, n):
        k, slot = self.index(up, n), self.slot(up, n)
        return remote(slot, slot, self.zs.at[k], self.zr.at[k], self.z_peer(up, 1))

    def along_x(self, up, n, way, src=None):
        k, slot = self.index(up, n), self.slot(up, n)
        peer = self.x_up if way == 0 else self.x_down
        return remote(slot if src is None else src, slot, self.xs.at[k, way], self.xr.at[k, way], peer)

    def far_x(self, up, n):
        k, slot = self.index(up, n), self.slot(up, n, 3 if up else 1)
        return remote(slot, slot, self.xs.at[k, 2], self.xr.at[k, 2], self.x_up if up else self.x_down)

    def across(self, up, n, core):
        k, row = self.index(up, n), self.buf.at[self.plane(up, n), :, core]
        return remote(row, row, self.ps.at[k], self.pr.at[k], self.partner)

    def each(self, n, work):
        when(n <= self.ups, lambda: work(True))
        when(n <= self.downs, lambda: work(False))

    def begin(self):
        own = self.own
        self.pass_on(True, 0, own)
        self.pass_on(False, 0, own)
        self.along_x(True, 0, 0, own).start()
        self.along_x(True, 0, 1, own).start()
        self.buf[self.z, self.x, self.c] = own[...]

    def step_z(self, n):
        def work(up):
            self.on_z(up, n).wait_recv()
            when(n % self.stride == 0, lambda: self.pass_on(up, n, self.slot(up, n)))
            for way in (0, 1):
                self.along_x(up, n, way).start()

        self.each(n, work)

    def step_x(self, n, first=False):
        def work(up):
            for way in (0, 1):
                self.along_x(up, n, way).wait_recv()
            self.far_x(up, n).start()

        work(True) if first else self.each(n, work)

    def step_far(self, n, first=False):
        def work(up):
            self.far_x(up, n).wait_recv()
            self.across(up, n, self.c).start()

        work(True) if first else self.each(n, work)

    def step_across(self, n, first=False):
        def work(up):
            self.across(up, n, 1 - self.c).wait_recv()

        work(True) if first else self.each(n, work)

    def finish(self):
        for k in range(self.nz):
            up = k <= self.ups
            n = k if up else k - self.ups
            if k:
                self.on_z(up, n).wait_send()
            for way in (0, 1):
                self.along_x(up, n, way).wait_send()
            self.far_x(up, n).wait_send()
            self.across(up, n, self.c).wait_send()


def remote(src, dst, ssem, rsem, peer):
    return pltpu.make_async_remote_copy(
        src_ref=src, dst_ref=dst, send_sem=ssem, recv_sem=rsem, device_id=peer, device_id_type=MESH
    )


def when(cond, work):
    if isinstance(cond, bool):
        if cond:
            work()
    else:
        pl.when(cond)(work)


def run(nets, waits):
    for one in waits:
        net, kind, n = nets[one[0]], one[1], int(one[2:])
        if kind == "b":
            net.begin()
        else:
            step = {"z": net.step_z, "x": net.step_x, "f": net.step_far, "p": net.step_across}[kind]
            step(n, *([] if n else [True]))


def greet(peers):
    barrier = pltpu.get_barrier_semaphore()
    for peer in peers:
        pl.semaphore_signal(barrier, inc=1, device_id=peer, device_id_type=MESH)
    pl.semaphore_wait(barrier, len(peers))


def spread_sems(nz):
    dma = pltpu.SemaphoreType.DMA
    return [dma((nz,)), dma((nz,)), dma((nz, 3)), dma((nz, 3)), dma((nz,)), dma((nz,))]


def layer_kernel(
    nz, nt, rows_ref, stream_ref, gain_ref, attn_ref, convw_ref, taps_ref, bias_ref, mixed_ref, weight_ref,
    rows_buf, kv_buf, out_buf, own_kv, own_out, heard, scaled, acc, q_ref, conv_ref, gate_ref,
    tri, halo, o_new, s_new, o_old, s_old, part, summed, *sems,
):
    nets = {
        "i": Spread(nz, 3, True, rows_ref, rows_buf, *sems[:6]),
        "k": Spread(nz, 2, False, own_kv, kv_buf, *sems[6:12]),
        "w": Spread(nz, 1, True, own_out, out_buf, *sems[12:18]),
    }
    net = nets["i"]
    ys, yr, hs, hr, ts, tr = sems[18:]
    project_order, attend_order, last_order = orders_of(nz)
    me = (net.z * 4 + net.x) * 2 + net.c
    y = lax.axis_index("tp")
    rows = stream_ref.shape[0]
    heads = bias_ref.shape[0]
    wide = conv_ref.shape[1]
    total = nz * 8
    share = nz // nt

    def device(index):
        return {"sp_0": lax.div(index, 8), "sp_1": lax.rem(lax.div(index, 2), 4), "sp_2": lax.rem(index, 2)}

    ahead, behind = device(lax.rem(me + 1, total)), device(lax.rem(me + total - 1, total))
    others = [{"tp": lax.rem(y + r, nt)} for r in range(1, nt)]
    greet((*net.peers, ahead, behind, *others))
    net.begin()
    sent = [
        remote(stream_ref, heard.at[y], ys.at[r], yr.at[r], others[r - 1]) for r in (2, 1, 3) if r < nt
    ]
    for one in sent:
        one.start()
    heard[y] = stream_ref[...]
    acc[...] = jnp.zeros_like(acc)
    for j in range(4):
        source = (attn_ref, convw_ref)[j // 2]
        own_out[pl.ds(16 * j, 16), :] = source[:, 128 * (j % 2) : 128 * (j % 2 + 1)]
    after = lax.broadcasted_iota(jnp.int32, tri.shape, 0) > lax.broadcasted_iota(jnp.int32, tri.shape, 1)
    tri[...] = jnp.where(after, 1.0, 0.0).astype(jnp.bfloat16)
    for ref in (o_new, s_new, o_old, s_old):
        ref[...] = jnp.zeros_like(ref)

    def scale():
        for r in range(1, nt):
            slot = heard.at[lax.rem(y + nt - r, nt)]
            remote(slot, slot, ys.at[r], yr.at[r], others[r - 1]).wait_recv()
        squares = jnp.zeros((rows, 1), jnp.float32)
        for b in range(nt):
            piece = heard[b].astype(jnp.float32)
            squares = squares + jnp.sum(piece * piece, axis=1, keepdims=True)
            piece = (piece * gain_ref[:, b * share * 128 : (b + 1) * share * 128]).astype(jnp.bfloat16)
            for j in range(share):
                scaled[b * share + j] = piece[:, 128 * j : 128 * (j + 1)]
        return squares

    def take_rows(up, n):
        at = net.plane(up, n)
        acc[...] += jnp.dot(
            scaled[at], rows_buf[at].reshape(128, acc.shape[1]), preferred_element_type=jnp.float32
        )

    squares = None
    for one in project_order:
        run(nets, [one])
        if one[:2] == "ip":
            n = int(one[2:])
            if n == 0:
                squares = scale()
            take_rows(True, n)
            if 0 < n <= net.downs:
                take_rows(False, n)
    row_scale = lax.rsqrt(squares / (nz * 128) + EPS)
    mine = (acc[...] * row_scale).astype(jnp.bfloat16)
    own_kv[...] = mine[:, : 2 * HEAD]
    conv_ref[...] = mine[:, 2 * HEAD + wide : 2 * HEAD + 2 * wide]
    gate_ref[...] = mine[:, 2 * HEAD + 2 * wide :]
    for h in range(heads):
        begin = 2 * HEAD + h * HEAD
        q = mine[:, begin : begin + HEAD].astype(jnp.float32) * (HEAD ** (-0.5) / LN2)
        high = q.astype(jnp.bfloat16).astype(jnp.float32)
        q_ref[pl.ds(h * rows, rows), :] = jnp.concatenate([high, q - high], axis=1).astype(jnp.bfloat16)
    nets["k"].begin()
    tail = remote(conv_ref.at[pl.ds(rows - 16, 16), :], halo, hs, hr, ahead)
    tail.start()

    def sweep(at, masked):
        gone, sticks, values = None, [], []
        for i in (3, 2, 1, 0):
            kv = kv_buf[at, i].reshape(KEYS, 2 * HEAD)
            both = jnp.concatenate([kv[:, :HEAD], kv[:, :HEAD]], axis=1)
            score = lax.dot_general(q_ref[...], both, NT, preferred_element_type=jnp.float32)
            score = jnp.concatenate(
                [score[h * rows : (h + 1) * rows] + bias_ref[h] / LN2 for h in range(heads)], axis=0
            )
            if masked:
                key_pos = i * KEYS + lax.broadcasted_iota(jnp.int32, score.shape, 1)
                query_pos = lax.rem(me, 8) * rows + lax.rem(
                    lax.broadcasted_iota(jnp.int32, score.shape, 0), rows
                )
                score = jnp.where(key_pos < query_pos, score, -1e30)
            fail = jnp.maximum(score, lax.log2(1.0 + jnp.exp2(jnp.minimum(score, 80.0))))
            later = jnp.dot(fail.astype(jnp.bfloat16), tri[...], preferred_element_type=jnp.float32)
            power = (score - fail) - later
            block = later[:, :1] + fail[:, :1]
            if gone is None:
                gone = jnp.broadcast_to(block, (heads * rows, 2 * HEAD))
            else:
                power = power - jnp.concatenate([gone, gone], axis=1)
                gone = gone + block
            sticks.append(jnp.exp2(power).astype(jnp.bfloat16))
            values.append(kv)
        out = jnp.dot(
            jnp.concatenate(sticks, axis=1),
            jnp.concatenate(values, axis=0),
            preferred_element_type=jnp.float32,
        )
        return out, gone

    def take_new(n, masked=False):
        out, gone = sweep(net.plane(True, n), masked)
        before = s_new[...]
        o_new[...] += jnp.exp2(-before) * out
        s_new[...] = before + gone

    def take_old(n):
        out, gone = sweep(net.plane(False, n), False)
        o_old[...] = o_old[...] * jnp.exp2(-gone) + out
        s_old[...] += gone

    run(nets, attend_order[0])
    take_new(0, True)

    def at_step(n, offset):
        for i in range(1, net.ups + 1):
            at = 2 * i - 1 + offset
            if at < len(attend_order) and attend_order[at]:
                pl.when(n == i)(functools.partial(run, nets, attend_order[at]))

    @pl.loop(1, net.ups + 1)
    def _(n):
        at_step(n, 0)
        pl.when(net.z - n >= 0)(lambda: take_new(n))
        at_step(n, 1)
        pl.when((net.z + n >= nz) & (n <= net.downs))(lambda: take_old(n))

    run(nets, last_order)
    gone = s_new[...]
    out = o_new[...] + jnp.exp2(-gone) * o_old[...]
    survived = (gone + s_old[...]) * LN2
    attended = [out[h * rows : (h + 1) * rows, HEAD:] for h in range(heads)]

    tail.wait_recv()
    now = conv_ref[...].astype(jnp.float32)
    last = halo[...].astype(jnp.float32) * jnp.where(me > 0, 1.0, 0.0)
    row = lax.broadcasted_iota(jnp.int32, now.shape, 0)
    one = jnp.where(row == 0, last[15:16], pltpu.roll(now, 1, 0))
    two = jnp.where(row == 0, last[14:15], jnp.where(row == 1, last[15:16], pltpu.roll(now, 2, 0)))
    conv = taps_ref[0:1, :] * two + taps_ref[1:2, :] * one + taps_ref[2:3, :] * now
    conv = gate_ref[...].astype(jnp.float32) * conv
    act = jnp.concatenate([*attended, conv], axis=1).astype(jnp.bfloat16)

    def project(to):
        planes = pl.ds(to * share, share)
        acc = None
        for j in range(4):
            w = out_buf[planes, :, :, pl.ds(16 * j, 16), :].reshape(share * 128, 128)
            term = lax.dot_general(
                act[:, 128 * j : 128 * (j + 1)], w, NT, preferred_element_type=jnp.float32
            )
            acc = term if acc is None else acc + term
        return acc.astype(jnp.bfloat16)

    parts = []
    for r in [*range(2, nt), 1] if nt > 1 else []:
        part[r] = project(lax.rem(y + r, nt))
        parts.append(remote(part.at[r], summed.at[r], ts.at[r], tr.at[r], others[r - 1]))
        parts[-1].start()
    mixed = project(y).astype(jnp.float32)
    weight = jnp.log(jnp.maximum(1.0 - jnp.exp(-survived), FLOOR))
    diagonal = lax.broadcasted_iota(jnp.int32, (rows, rows), 0) == lax.broadcasted_iota(
        jnp.int32, (rows, rows), 1
    )
    for h in range(heads):
        weight_ref[pl.ds(h, 1), :] = jnp.sum(
            jnp.where(diagonal, weight[h * rows : (h + 1) * rows], 0.0), axis=0, keepdims=True
        )
    for one in sent:
        one.wait_send()
    tail.wait_send()
    for each in nets.values():
        each.finish()
    for one in parts:
        one.wait_recv()
    for r in range(1, nt):
        mixed = mixed + summed[r].astype(jnp.float32)
    mixed_ref[...] = mixed.astype(jnp.bfloat16)
    for one in parts:
        one.wait_send()


def layer(rows, stream, norm_gain, w_out_attn, w_out_conv, conv_taps, sb_bias, nz, nt):
    tokens = stream.shape[0]
    heads = sb_bias.shape[0]
    wide = heads * HEAD
    vmem = pl.BlockSpec(memory_space=pltpu.VMEM)
    dma = pltpu.SemaphoreType.DMA
    half = lambda *shape: pltpu.VMEM(shape, jnp.bfloat16)
    sums = pltpu.VMEM((heads * tokens, 2 * HEAD), jnp.float32)
    return pl.pallas_call(
        functools.partial(layer_kernel, nz, nt),
        name="layer",
        out_shape=(
            jax.ShapeDtypeStruct(stream.shape, jnp.bfloat16),
            jax.ShapeDtypeStruct((heads, tokens), jnp.float32),
        ),
        in_specs=[vmem] * 6 + [pl.BlockSpec(memory_space=pltpu.SMEM)],
        out_specs=(vmem, vmem),
        scratch_shapes=[
            half(nz, 4, 2, *rows.shape),
            half(nz, 4, 2, tokens, 2 * HEAD),
            half(nz, 4, 2, 64, 128),
            half(tokens, 2 * HEAD),
            half(64, 128),
            half(nt, *stream.shape),
            half(nz, tokens, 128),
            pltpu.VMEM((tokens, rows.shape[1]), jnp.float32),
            half(heads * tokens, 2 * HEAD),
            half(tokens, wide),
            half(tokens, wide),
            half(KEYS, KEYS),
            half(16, wide),
            *[sums] * 4,
            *[half(nt, *stream.shape)] * 2,
            *spread_sems(nz),
            *spread_sems(nz),
            *spread_sems(nz),
            dma((nt,)),
            dma((nt,)),
            dma,
            dma,
            dma((nt,)),
            dma((nt,)),
        ],
        compiler_params=pltpu.CompilerParams(collective_id=0, has_side_effects=True),
    )(rows, stream, norm_gain[None, :], w_out_attn.T, w_out_conv.T, conv_taps, sb_bias)


def local(
    stream,
    norm_gain,
    w_query,
    w_key,
    w_value,
    w_conv_in,
    w_conv_gate,
    conv_taps,
    sb_bias,
    w_out_attn,
    w_out_conv,
):
    nz, nt = lax.axis_size(SP[0]), lax.axis_size("tp")
    rows = jnp.concatenate([w_key, w_value, w_query, w_conv_in, w_conv_gate], axis=1)
    return layer(rows, stream, norm_gain, w_out_attn, w_out_conv, conv_taps, sb_bias, nz, nt)


def solution(mesh):
    torus = Mesh(
        mesh.devices.reshape(mesh.shape["sp"] // 8, 4, 2, mesh.shape["tp"]),
        ("sp_0", "sp_1", "sp_2", "tp"),
    )
    return jax.shard_map(
        local,
        mesh=torus,
        in_specs=(
            P(SP, "tp"),
            P(),
            P(SP, "tp"),
            P(SP, "tp"),
            P(SP, "tp"),
            P(SP, "tp"),
            P(SP, "tp"),
            P(None, "tp"),
            P("tp"),
            P("tp", SP),
            P("tp", SP),
        ),
        out_specs=(P(SP, "tp"), P("tp", SP)),
        check_vma=False,
    )
```

```python
import functools

import jax
import jax.numpy as jnp
from jax import lax
from jax.experimental import pallas as pl
from jax.experimental.pallas import tpu as pltpu
from jax.sharding import Mesh
from jax.sharding import PartitionSpec as P

HEAD = 64
SP = ("sp_0", "sp_1", "sp_2")
KEYS = 256
EPS = 1e-06
FLOOR = 0.02
LN2 = 0.6931471805599453
NT = (((1,), (1,)), ((), ()))
MESH = pl.DeviceIdType.MESH


PROJECT_ORDER = (
    "ix0", "iz3", "iz1", "iz2", "if0", "ip0", "ix3", "ix1", "iz6", "iz4", "ix2", "iz5",
    "if3", "if1", "ip3", "ix6", "ip1", "iz7", "iz8", "wb0", "ix4", "if2", "ix5", "ip2",
    "if6", "wz1", "ix7", "ip6", "ix8", "wx0", "if4", "if5", "wz2", "wx1", "ip4", "if7",
    "ip5", "if8", "wf0", "ip7", "wz3", "ip8",
)
ATTEND_ORDER = (
    ("wx2", "wf1", "wp0", "wp1", "wz4", "wx3", "kz1", "kx0", "wf2", "wx4", "wz5", "wp2", "wf3", "kz2", "wp3", "kx1", "kf0", "wz6", "wf4", "kz3", "wx5", "kp0",),
    ("kz4", "kx2", "kf1", "wz7", "wp4", "wx6", "kp1",),
    ("kx3", "wf5",),
    ("kz5", "kx4", "kf2", "wp5", "wz8", "wx7", "kz6", "wf6", "kp2",),
    ("kf3", "wp6",),
    ("kz7", "kx5", "kf4", "kp3",),
    ("kz8", "wx8", "kp4", "wf7",),
    ("kx6", "wp7",),
    ("kx7", "kf5",),
    ("kx8", "wf8", "kp5",),
    ("kf6", "wp8",),
    ("kf7", "kp6",),
    ("kf8", "kp7",),
    ("kp8",),
    (),
    (),
)
LAST_ORDER = ()


def orders_of(nz):
    if nz == 16:
        return PROJECT_ORDER, ATTEND_ORDER, LAST_ORDER
    ups, downs = nz // 2, (nz - 1) // 2
    first = lambda s: [s + kind + "0" for kind in "xfp"]
    waits = lambda s, n: [s + kind + str(n) for kind in "zxfp"]
    rows = [*first("i"), *(one for n in range(1, ups + 1) for one in waits("i", n))]
    keys = [first("k")]
    for n in range(1, ups + 1):
        keys += [waits("k", n), *[[]] * (n <= downs)]
    last = ["wb0", *first("w"), *(one for n in range(1, ups + 1) for one in waits("w", n))]
    return rows, keys, last


class Spread:
    def __init__(self, nz, stride, far_first, own, buf, zs, zr, xs, xr, fr, ps, pr):
        self.nz, self.own, self.buf = nz, own, buf
        self.zs, self.zr, self.xs, self.xr, self.fr, self.ps, self.pr = zs, zr, xs, xr, fr, ps, pr
        self.z, self.x, self.c = (lax.axis_index(a) for a in SP)
        self.ups, self.downs = nz // 2, (nz - 1) // 2
        self.stride = min(stride, self.ups)
        self.reach = [*range(1, self.stride + 1)][:: -1 if far_first else 1]
        self.x_up, self.x_down = ({"sp_1": lax.rem(self.x + d, 4)} for d in (1, 3))
        self.partner = {"sp_2": 1 - self.c}
        on_z = [self.z_peer(up, r) for r in range(1, self.stride + 1) for up in (True, False)]
        self.peers = (*on_z, self.x_up, self.x_down, self.partner)

    def z_peer(self, up, r):
        return {"sp_0": lax.rem(self.z + r if up else self.z - r + self.nz, self.nz)}

    def limit(self, up):
        return self.ups if up else self.downs

    def plane(self, up, n):
        return lax.rem(self.z - n + self.nz, self.nz) if up else lax.rem(self.z + n, self.nz)

    def slot(self, up, n, dx=0):
        return self.buf.at[self.plane(up, n), lax.rem(self.x + dx, 4), self.c]

    def index(self, up, n):
        return n if up else self.ups + n

    def pass_on(self, up, n, src):
        for r in self.reach:
            k, slot = self.index(up, n + r), self.slot(up, n)
            sems = self.zs, self.zr.at[k]
            if n + r <= self.limit(up):
                remote(src, slot, *sems, self.z_peer(up, r)).start()

    def on_z(self, up, n):
        k, slot = self.index(up, n), self.slot(up, n)
        return remote(slot, slot, self.zs, self.zr.at[k], self.z_peer(up, 1))

    def along_x(self, up, n, way, src=None):
        slot = self.slot(up, n)
        peer = self.x_up if way == 0 else self.x_down
        return remote(slot if src is None else src, slot, self.xs, self.xr.at[n], peer)

    def far_x(self, up, n):
        slot = self.slot(up, n, 3 if up else 1)
        return remote(slot, slot, self.xs, self.fr.at[n], self.x_up if up else self.x_down)

    def across(self, up, n):
        row = self.buf.at[self.plane(up, n), :, self.c]
        return remote(row, row, self.ps, self.pr.at[n], self.partner)

    def rings(self, n):
        return [True] * (n <= self.ups) + [False] * (0 < n <= self.downs)

    def arrived(self, like, rsem):
        remote(like, like, self.xs, rsem, self.partner).wait_recv()

    def left(self, like, ssem):
        remote(like, like, ssem, self.zr.at[0], self.partner).wait_send()

    def begin(self):
        own = self.own
        self.pass_on(True, 0, own)
        self.pass_on(False, 0, own)
        self.along_x(True, 0, 0, own).start()
        self.along_x(True, 0, 1, own).start()
        self.buf[self.z, self.x, self.c] = own[...]

    def step_z(self, n):
        for up in self.rings(n):
            self.on_z(up, n).wait_recv()
            if n % self.stride == 0:
                self.pass_on(up, n, self.slot(up, n))
            for way in (0, 1):
                self.along_x(up, n, way).start()

    def step_x(self, n):
        rings = self.rings(n)
        if rings:
            self.arrived(self.buf.at[0, pl.ds(0, 2 * len(rings)), self.c], self.xr.at[n])
        for up in rings:
            self.far_x(up, n).start()

    def step_far(self, n):
        rings = self.rings(n)
        if rings:
            self.arrived(self.buf.at[0, pl.ds(0, len(rings)), self.c], self.fr.at[n])
        for up in rings:
            self.across(up, n).start()

    def step_across(self, n):
        rings = self.rings(n)
        if rings:
            self.arrived(self.buf.at[pl.ds(0, len(rings)), :, 1 - self.c], self.pr.at[n])

    def finish(self):
        self.left(self.buf.at[pl.ds(0, self.nz - 1), 0, 0], self.zs)
        self.left(self.buf.at[:, pl.ds(0, 3), 0], self.xs)
        self.left(self.buf.at[:, :, 0], self.ps)


def remote(src, dst, ssem, rsem, peer):
    return pltpu.make_async_remote_copy(
        src_ref=src, dst_ref=dst, send_sem=ssem, recv_sem=rsem, device_id=peer, device_id_type=MESH
    )


def run(nets, waits):
    for one in waits:
        net, kind, n = nets[one[0]], one[1], int(one[2:])
        if kind == "b":
            net.begin()
        else:
            step = {"z": net.step_z, "x": net.step_x, "f": net.step_far, "p": net.step_across}[kind]
            step(n)


def greet(peers):
    barrier = pltpu.get_barrier_semaphore()
    for peer in peers:
        pl.semaphore_signal(barrier, inc=1, device_id=peer, device_id_type=MESH)
    pl.semaphore_wait(barrier, len(peers))


def spread_sems(nz):
    dma, steps = pltpu.SemaphoreType.DMA, nz // 2 + 1
    return [dma, dma((nz,)), dma, dma((steps,)), dma((steps,)), dma, dma((steps,))]


def layer_kernel(
    nz, nt, rows_ref, stream_ref, gain_ref, attn_ref, convw_ref, taps_ref, bias_ref, mixed_ref, weight_ref,
    rows_buf, kv_buf, out_buf, own_kv, own_out, heard, scaled, acc, q_ref, conv_ref, gate_ref,
    tri, halo, o_new, s_new, o_old, s_old, part, summed, *sems,
):
    nets = {
        "i": Spread(nz, 3, True, rows_ref, rows_buf, *sems[:7]),
        "k": Spread(nz, 2, False, own_kv, kv_buf, *sems[7:14]),
        "w": Spread(nz, 1, True, own_out, out_buf, *sems[14:21]),
    }
    net = nets["i"]
    ys, yr, hs, hr, ts, tr = sems[21:]
    project_order, attend_order, last_order = orders_of(nz)
    me = (net.z * 4 + net.x) * 2 + net.c
    y = lax.axis_index("tp")
    rows = stream_ref.shape[0]
    heads = bias_ref.shape[0]
    wide = conv_ref.shape[1]
    total = nz * 8
    share = nz // nt

    def device(index):
        return {"sp_0": lax.div(index, 8), "sp_1": lax.rem(lax.div(index, 2), 4), "sp_2": lax.rem(index, 2)}

    ahead, behind = device(lax.rem(me + 1, total)), device(lax.rem(me + total - 1, total))
    others = [{"tp": lax.rem(y + r, nt)} for r in range(1, nt)]
    greet((*net.peers, ahead, behind, *others))
    net.begin()
    sent = [
        remote(stream_ref, heard.at[y], ys.at[r], yr.at[r], others[r - 1]) for r in (2, 1, 3) if r < nt
    ]
    for one in sent:
        one.start()
    heard[y] = stream_ref[...]
    acc[...] = jnp.zeros_like(acc)
    for j in range(4):
        source = (attn_ref, convw_ref)[j // 2]
        own_out[pl.ds(16 * j, 16), :] = source[:, 128 * (j % 2) : 128 * (j % 2 + 1)]
    after = lax.broadcasted_iota(jnp.int32, tri.shape, 0) > lax.broadcasted_iota(jnp.int32, tri.shape, 1)
    tri[...] = jnp.where(after, 1.0, 0.0).astype(jnp.bfloat16)
    for ref in (o_new, s_new, o_old, s_old):
        ref[...] = jnp.zeros_like(ref)

    def scale():
        for r in range(1, nt):
            slot = heard.at[lax.rem(y + nt - r, nt)]
            remote(slot, slot, ys.at[r], yr.at[r], others[r - 1]).wait_recv()
        squares = jnp.zeros((rows, 1), jnp.float32)
        for b in range(nt):
            piece = heard[b].astype(jnp.float32)
            squares = squares + jnp.sum(piece * piece, axis=1, keepdims=True)
            piece = (piece * gain_ref[:, b * share * 128 : (b + 1) * share * 128]).astype(jnp.bfloat16)
            for j in range(share):
                scaled[b * share + j] = piece[:, 128 * j : 128 * (j + 1)]
        return squares

    def take_rows(up, n):
        at = net.plane(up, n)
        acc[...] += jnp.dot(
            scaled[at], rows_buf[at].reshape(128, acc.shape[1]), preferred_element_type=jnp.float32
        )

    squares = None
    for one in project_order:
        run(nets, [one])
        if one[:2] == "ip":
            n = int(one[2:])
            if n == 0:
                squares = scale()
            take_rows(True, n)
            if 0 < n <= net.downs:
                take_rows(False, n)
    row_scale = lax.rsqrt(squares / (nz * 128) + EPS)
    mine = (acc[...] * row_scale).astype(jnp.bfloat16)
    own_kv[...] = mine[:, : 2 * HEAD]
    conv_ref[...] = mine[:, 2 * HEAD + wide : 2 * HEAD + 2 * wide]
    gate_ref[...] = mine[:, 2 * HEAD + 2 * wide :]
    for h in range(heads):
        begin = 2 * HEAD + h * HEAD
        q = mine[:, begin : begin + HEAD].astype(jnp.float32) * (HEAD ** (-0.5) / LN2)
        high = q.astype(jnp.bfloat16).astype(jnp.float32)
        q_ref[pl.ds(h * rows, rows), :] = jnp.concatenate([high, q - high], axis=1).astype(jnp.bfloat16)
    nets["k"].begin()
    tail = remote(conv_ref.at[pl.ds(rows - 16, 16), :], halo, hs, hr, ahead)
    tail.start()

    def sweep(at, masked):
        gone, sticks, values = None, [], []
        for i in (3, 2, 1, 0):
            kv = kv_buf[at, i].reshape(KEYS, 2 * HEAD)
            both = jnp.concatenate([kv[:, :HEAD], kv[:, :HEAD]], axis=1)
            score = lax.dot_general(q_ref[...], both, NT, preferred_element_type=jnp.float32)
            score = jnp.concatenate(
                [score[h * rows : (h + 1) * rows] + bias_ref[h] / LN2 for h in range(heads)], axis=0
            )
            if masked:
                key_pos = i * KEYS + lax.broadcasted_iota(jnp.int32, score.shape, 1)
                query_pos = lax.rem(me, 8) * rows + lax.rem(
                    lax.broadcasted_iota(jnp.int32, score.shape, 0), rows
                )
                score = jnp.where(key_pos < query_pos, score, -1e30)
            fail = jnp.maximum(score, lax.log2(1.0 + jnp.exp2(jnp.minimum(score, 80.0))))
            later = jnp.dot(fail.astype(jnp.bfloat16), tri[...], preferred_element_type=jnp.float32)
            power = (score - fail) - later
            block = later[:, :1] + fail[:, :1]
            if gone is None:
                gone = jnp.broadcast_to(block, (heads * rows, 2 * HEAD))
            else:
                power = power - jnp.concatenate([gone, gone], axis=1)
                gone = gone + block
            sticks.append(jnp.exp2(power).astype(jnp.bfloat16))
            values.append(kv)
        out = jnp.dot(
            jnp.concatenate(sticks, axis=1),
            jnp.concatenate(values, axis=0),
            preferred_element_type=jnp.float32,
        )
        return out, gone

    def take_new(n, masked=False):
        out, gone = sweep(net.plane(True, n), masked)
        before = s_new[...]
        o_new[...] += jnp.exp2(-before) * out
        s_new[...] = before + gone

    def take_old(n):
        out, gone = sweep(net.plane(False, n), False)
        o_old[...] = o_old[...] * jnp.exp2(-gone) + out
        s_old[...] += gone

    run(nets, attend_order[0])
    take_new(0, True)

    def at_step(n, offset):
        for i in range(1, net.ups + 1):
            at = 2 * i - 1 + offset
            if at < len(attend_order) and attend_order[at]:
                pl.when(n == i)(functools.partial(run, nets, attend_order[at]))

    @pl.loop(1, net.ups + 1)
    def _(n):
        at_step(n, 0)
        pl.when(net.z - n >= 0)(lambda: take_new(n))
        at_step(n, 1)
        pl.when((net.z + n >= nz) & (n <= net.downs))(lambda: take_old(n))

    run(nets, last_order)
    gone = s_new[...]
    out = o_new[...] + jnp.exp2(-gone) * o_old[...]
    survived = (gone + s_old[...]) * LN2
    attended = [out[h * rows : (h + 1) * rows, HEAD:] for h in range(heads)]

    tail.wait_recv()
    now = conv_ref[...].astype(jnp.float32)
    last = halo[...].astype(jnp.float32) * jnp.where(me > 0, 1.0, 0.0)
    row = lax.broadcasted_iota(jnp.int32, now.shape, 0)
    one = jnp.where(row == 0, last[15:16], pltpu.roll(now, 1, 0))
    two = jnp.where(row == 0, last[14:15], jnp.where(row == 1, last[15:16], pltpu.roll(now, 2, 0)))
    conv = taps_ref[0:1, :] * two + taps_ref[1:2, :] * one + taps_ref[2:3, :] * now
    conv = gate_ref[...].astype(jnp.float32) * conv
    act = jnp.concatenate([*attended, conv], axis=1).astype(jnp.bfloat16)

    def project(to):
        planes = pl.ds(to * share, share)
        acc = None
        for j in range(4):
            w = out_buf[planes, :, :, pl.ds(16 * j, 16), :].reshape(share * 128, 128)
            term = lax.dot_general(
                act[:, 128 * j : 128 * (j + 1)], w, NT, preferred_element_type=jnp.float32
            )
            acc = term if acc is None else acc + term
        return acc.astype(jnp.bfloat16)

    parts = []
    for r in [*range(2, nt), 1] if nt > 1 else []:
        part[r] = project(lax.rem(y + r, nt))
        parts.append(remote(part.at[r], summed.at[r], ts.at[r], tr.at[r], others[r - 1]))
        parts[-1].start()
    mixed = project(y).astype(jnp.float32)
    weight = jnp.log(jnp.maximum(1.0 - jnp.exp(-survived), FLOOR))
    diagonal = lax.broadcasted_iota(jnp.int32, (rows, rows), 0) == lax.broadcasted_iota(
        jnp.int32, (rows, rows), 1
    )
    for h in range(heads):
        weight_ref[pl.ds(h, 1), :] = jnp.sum(
            jnp.where(diagonal, weight[h * rows : (h + 1) * rows], 0.0), axis=0, keepdims=True
        )
    for one in sent:
        one.wait_send()
    tail.wait_send()
    for each in nets.values():
        each.finish()
    for one in parts:
        one.wait_recv()
    for r in range(1, nt):
        mixed = mixed + summed[r].astype(jnp.float32)
    mixed_ref[...] = mixed.astype(jnp.bfloat16)
    for one in parts:
        one.wait_send()


def layer(rows, stream, norm_gain, w_out_attn, w_out_conv, conv_taps, sb_bias, nz, nt):
    tokens = stream.shape[0]
    heads = sb_bias.shape[0]
    wide = heads * HEAD
    vmem = pl.BlockSpec(memory_space=pltpu.VMEM)
    dma = pltpu.SemaphoreType.DMA
    half = lambda *shape: pltpu.VMEM(shape, jnp.bfloat16)
    sums = pltpu.VMEM((heads * tokens, 2 * HEAD), jnp.float32)
    return pl.pallas_call(
        functools.partial(layer_kernel, nz, nt),
        name="layer",
        out_shape=(
            jax.ShapeDtypeStruct(stream.shape, jnp.bfloat16),
            jax.ShapeDtypeStruct((heads, tokens), jnp.float32),
        ),
        in_specs=[vmem] * 6 + [pl.BlockSpec(memory_space=pltpu.SMEM)],
        out_specs=(vmem, vmem),
        scratch_shapes=[
            half(nz, 4, 2, *rows.shape),
            half(nz, 4, 2, tokens, 2 * HEAD),
            half(nz, 4, 2, 64, 128),
            half(tokens, 2 * HEAD),
            half(64, 128),
            half(nt, *stream.shape),
            half(nz, tokens, 128),
            pltpu.VMEM((tokens, rows.shape[1]), jnp.float32),
            half(heads * tokens, 2 * HEAD),
            half(tokens, wide),
            half(tokens, wide),
            half(KEYS, KEYS),
            half(16, wide),
            *[sums] * 4,
            *[half(nt, *stream.shape)] * 2,
            *spread_sems(nz),
            *spread_sems(nz),
            *spread_sems(nz),
            dma((nt,)),
            dma((nt,)),
            dma,
            dma,
            dma((nt,)),
            dma((nt,)),
        ],
        compiler_params=pltpu.CompilerParams(collective_id=0, has_side_effects=True),
    )(rows, stream, norm_gain[None, :], w_out_attn.T, w_out_conv.T, conv_taps, sb_bias)


def local(
    stream,
    norm_gain,
    w_query,
    w_key,
    w_value,
    w_conv_in,
    w_conv_gate,
    conv_taps,
    sb_bias,
    w_out_attn,
    w_out_conv,
):
    nz, nt = lax.axis_size(SP[0]), lax.axis_size("tp")
    rows = jnp.concatenate([w_key, w_value, w_query, w_conv_in, w_conv_gate], axis=1)
    return layer(rows, stream, norm_gain, w_out_attn, w_out_conv, conv_taps, sb_bias, nz, nt)


def solution(mesh):
    torus = Mesh(
        mesh.devices.reshape(mesh.shape["sp"] // 8, 4, 2, mesh.shape["tp"]),
        ("sp_0", "sp_1", "sp_2", "tp"),
    )
    return jax.shard_map(
        local,
        mesh=torus,
        in_specs=(
            P(SP, "tp"),
            P(),
            P(SP, "tp"),
            P(SP, "tp"),
            P(SP, "tp"),
            P(SP, "tp"),
            P(SP, "tp"),
            P(None, "tp"),
            P("tp"),
            P("tp", SP),
            P("tp", SP),
        ),
        out_specs=(P(SP, "tp"), P("tp", SP)),
        check_vma=False,
    )
```
